256 devices in a mesh: ep: 16 (over y, x), tp: 16 (over z, core).
Axes of the slice: x: 4, y: 4, z: 8, core: 2. Of those that a mesh axis runs over, the one named last changes fastest.
Arguments:
- q_latent: bfloat16 [12288, 384], P(('ep', 'tp')), may hold values from -6 to 6
- kv_latent: bfloat16 [12288, 256], P(('ep', 'tp')), may hold values from -6 to 6
- rope_key: bfloat16 [12288, 64], P(('ep', 'tp')), may hold values from -6 to 6
- q_latent_gain: float32 [384], replicated, may hold values from 0.1 to 1.9
- kv_latent_gain: float32 [256], replicated, may hold values from 0.1 to 1.9
- w_query: bfloat16 [384, 3072], P(None, 'tp'), may hold values from -0.3125 to 0.3125
- w_key: bfloat16 [256, 2048], P(None, 'tp'), may hold values from -0.375 to 0.375
- w_value: bfloat16 [256, 2048], P(None, 'tp'), may hold values from -0.375 to 0.375
- query_gain: float32 [192], replicated, may hold values from 0.1 to 1.9
- key_gain: float32 [192], replicated, may hold values from 0.1 to 1.9
- w_mix: bfloat16 [2048, 2048], P('tp'), may hold values from -3 to 3
- tokens_b: bfloat16 [12288, 2048], P(('ep', 'tp')), may hold values from -6 to 6
- norm_gain: float32 [2048], replicated, may hold values from 0.1 to 1.9
- expert_ids: int32 [12288, 2], P(('ep', 'tp')), may hold values from 0 to 31, all different within a row; in each aligned block of 48 rows (0 to 47, 48 to 95, ...) at most 4 rows name the same one
- route_weights: float32 [12288, 2], P(('ep', 'tp')), may hold values from 0.05 to 1
- w_gate: bfloat16 [32, 2048, 4096], P('ep', None, 'tp'), may hold values from -0.125 to 0.125
- w_up: bfloat16 [32, 2048, 4096], P('ep', None, 'tp'), may hold values from -0.125 to 0.125
- w_down: bfloat16 [32, 4096, 2048], P('ep', 'tp'), may hold values from -0.09375 to 0.09375
Outputs:
- mix_out: bfloat16 [12288, 2048], P(('ep', 'tp'))
- expert_out: bfloat16 [12288, 2048], P(('ep', 'tp'))
The draws below stay inside these ranges and needn't reach their ends.
Inputs may be any that keep to these rules, and one draw needn't show every extreme that they name: `expert_ids`: each row names 2 different experts. Within the rows of one device, no expert is named more than 4 times, a bound that some block reaches.
All inputs are finite; a program needn't handle non-finite values.
Results may differ from the reference program's by a relative error of at most 0.018.
Values may be sent and summed in bfloat16 or wider, within the bound.
No kernel may reach another device: no remote copies, remote signals or barrier semaphores. Data moves between devices by JAX's collectives and lax.ppermute only.
A program may use at most 192 MiB of HBM per device.

```python
import math
import jax
import jax.numpy as jnp
import numpy as np
from jax import lax

MODEL_DIM = 2048
HEADS = 16
Q_RANK = 384
KV_RANK = 256
NOPE_DIM = 128
ROPE_DIM = 64
VALUE_DIM = 128
EXPERTS = 32
FF_DIM = 4096
TOP_K = 2
ROWS = 768
TOKENS = 12288
CAP_SLOTS = 4
N_EP = 16
N_TP = 16


def levels(key, shape, shards, low, top_value):
    factor_of, own = 1.0, jax.random.fold_in(key, 6)
    for position, parts in shards:
        draws = jnp.exp(jax.random.uniform(jax.random.fold_in(own, position), (parts,), jnp.float32, low / len(shards), top_value / len(shards)))
        factor_of = factor_of * jnp.repeat(draws, shape[position] // parts).reshape([-1 if axis == position else 1 for axis in range(len(shape))])
    return factor_of


def deal_out(stream_key, own, number, rows, count, top, bound, lean):
    sequence = jax.random.permutation(stream_key, count)
    heavy_load, common = shares(count, rows * top, bound, lean, True), shares(count, rows * top, bound, lean, False)
    places = jnp.arange(count)

    def named(sizes, offset_by):
        used = int((sizes > 0).sum())
        fixed = max(1, used // 4)
        moved = fixed + (places - fixed + offset_by * (used - fixed)) % max(1, count - fixed)
        return jnp.zeros((count,), jnp.int32).at[sequence[jnp.where(places < fixed, places, moved)]].set(jnp.asarray(sizes, jnp.int32))

    sizes = jnp.where(number % 4 == 0, named(heavy_load, number // 4), named(common, number - number // 4 - 1))
    mixed = jax.random.permutation(jax.random.fold_in(own, 3), count)
    donor, sink = mixed[0:count // 2 * 2:2], mixed[1:count // 2 * 2:2]
    margin = jnp.minimum(sizes[donor] - 1, bound - sizes[sink]) // 2
    margin = jnp.where((donor == sequence[0]) | (sink == sequence[0]) | (sizes[sink] == 0), 0, jnp.maximum(margin, 0))
    moved = jax.random.randint(jax.random.fold_in(own, 4), (count // 2,), 0, 1 << 20) % (margin + 1)
    sizes = sizes.at[donor].add(-moved).at[sink].add(moved)
    members = jnp.searchsorted(jnp.cumsum(sizes), jnp.arange(rows * top), side="right").astype(jnp.int32)
    grid = members.reshape(top, rows).T
    grid = grid[jax.random.permutation(jax.random.fold_in(own, 1), rows)]
    offset_by = jax.random.randint(jax.random.fold_in(own, 2), (rows, 1), 0, top)
    return jnp.take_along_axis(grid, (jnp.arange(top)[None, :] + offset_by) % top, axis=1)


def shares(amount, total, reach, lean, full):
    portions = [(1 << 20) // math.isqrt(grade ** lean) + 1 for grade in range(1, amount + 1)]
    largest = reach if full else min(reach, max(-(-total // amount), total * portions[0] // sum(portions)))
    least = 1 if total - largest >= amount - 1 else 0
    counts, spare = [largest] + [least] * (amount - 1), total - largest - least * (amount - 1)
    while spare > 0:
        movable = [i for i in range(1, amount) if counts[i] < largest] or [i for i in range(1, amount) if counts[i] < reach]
        whole, left = sum([portions[i] for i in movable]), spare
        for i in movable:
            extra = min(reach - counts[i], max(1, left * portions[i] // whole), spare)
            counts[i] = counts[i] + extra
            spare = spare - extra
    return np.array(counts)


def noise(rng, shape, width, reach, split=(), kind=jnp.bfloat16):
    values = jax.random.normal(rng, shape, jnp.float32) * width
    if len(split) > 0:
        values = levels(rng, shape, split, -0.22, 0.18) * values
    return jnp.clip(values, min=-reach, max=reach).astype(kind)


def setup_inputs(seed: int = 0) -> dict:
    splits = jax.random.split(jax.random.key(seed), 19)
    q_latent = noise(splits[0], (TOKENS, Q_RANK), 1.0, 6.0, ((0, 256),))
    kv_latent = noise(splits[1], (TOKENS, KV_RANK), 1.0, 6.0, ((0, 256),))
    rope_key = noise(splits[2], (TOKENS, ROPE_DIM), 1.0, 6.0, ((0, 256),))
    q_latent_gain = jnp.clip(1.0 + 0.18 * jax.random.normal(splits[3], (Q_RANK,), jnp.float32), 0.1, 1.9)
    kv_latent_gain = jnp.clip(1.0 + 0.18 * jax.random.normal(splits[4], (KV_RANK,), jnp.float32), 0.1, 1.9)
    w_query = noise(splits[5], (Q_RANK, HEADS * (NOPE_DIM + ROPE_DIM)), Q_RANK ** -0.5, 0.3125, ((1, 16),))
    w_key = noise(splits[6], (KV_RANK, HEADS * NOPE_DIM), KV_RANK ** -0.5, 0.375, ((1, 16),))
    w_value = noise(splits[7], (KV_RANK, HEADS * VALUE_DIM), KV_RANK ** -0.5, 0.375, ((1, 16),))
    query_gain = jnp.clip(1.0 + 0.18 * jax.random.normal(splits[8], (NOPE_DIM + ROPE_DIM,), jnp.float32), 0.1, 1.9)
    key_gain = jnp.clip(1.0 + 0.18 * jax.random.normal(splits[9], (NOPE_DIM + ROPE_DIM,), jnp.float32), 0.1, 1.9)
    w_mix = noise(splits[10], (HEADS * VALUE_DIM, MODEL_DIM), 0.5, 3.0, ((0, 16),))
    tokens_b = noise(splits[11], (TOKENS, MODEL_DIM), 1.0, 6.0, ((0, 256),))
    norm_gain = jnp.clip(1.0 + 0.18 * jax.random.normal(splits[12], (MODEL_DIM,), jnp.float32), 0.1, 1.9)
    expert_ids_keys = jax.random.split(jax.random.fold_in(splits[13], 1), TOKENS // (ROWS // N_TP))
    expert_ids_turns = jax.random.permutation(jax.random.fold_in(splits[13], 3), TOKENS // (ROWS // N_TP))
    expert_ids = jax.vmap(lambda own, number: deal_out(jax.random.fold_in(splits[13], 2), own, number, ROWS // N_TP, EXPERTS, TOP_K, CAP_SLOTS, 1))(expert_ids_keys, expert_ids_turns).reshape((TOKENS, TOP_K))
    route_weights = jnp.clip(jnp.exp(math.log(1.0) - 2.9957323 * jax.random.uniform(splits[14], (TOKENS, TOP_K), jnp.float32) ** levels(splits[14], (TOKENS, TOP_K), ((0, 256),), -0.2, 0.2)), 0.05, 1.0)
    w_gate = noise(splits[15], (EXPERTS, MODEL_DIM, FF_DIM), MODEL_DIM ** -0.5, 0.125, ((0, 16), (2, 16)))
    w_up = noise(splits[16], (EXPERTS, MODEL_DIM, FF_DIM), MODEL_DIM ** -0.5, 0.125, ((0, 16), (2, 16)))
    w_down = noise(splits[17], (EXPERTS, FF_DIM, MODEL_DIM), FF_DIM ** -0.5, 0.09375, ((0, 16), (1, 16)))
    return {"q_latent": q_latent, "kv_latent": kv_latent, "rope_key": rope_key, "q_latent_gain": q_latent_gain, "kv_latent_gain": kv_latent_gain, "w_query": w_query, "w_key": w_key, "w_value": w_value, "query_gain": query_gain, "key_gain": key_gain, "w_mix": w_mix, "tokens_b": tokens_b, "norm_gain": norm_gain, "expert_ids": expert_ids, "route_weights": route_weights, "w_gate": w_gate, "w_up": w_up, "w_down": w_down}


EPSILON = 1e-06
THETA = 10000.0

def rms_scale(values, gains):
    return values * lax.rsqrt(lax.optimization_barrier(jnp.mean(values * values, axis=-1, keepdims=True)) + EPSILON) * gains

def rotate(values, positions):
    half_dim = values.shape[-1] // 2
    inverse = THETA ** (-jnp.arange(0, 2 * half_dim, 2, dtype=jnp.float32) / (2 * half_dim))
    angles = positions.astype(jnp.float32)[:, None] * inverse[None, :]
    view_shape = (positions.shape[0],) + (1,) * (values.ndim - 2) + (half_dim,)
    cosine = jnp.cos(angles).reshape(view_shape)
    sine_part = jnp.sin(angles).reshape(view_shape)
    first_half = values[..., :half_dim]
    second = values[..., half_dim:]
    return jnp.concatenate([first_half * cosine - second * sine_part, second * cosine + first_half * sine_part], axis=-1)

def reference(q_latent, kv_latent, rope_key, q_latent_gain, kv_latent_gain, w_query, w_key, w_value, query_gain, key_gain, w_mix, tokens_b, norm_gain, expert_ids, route_weights, w_gate, w_up, w_down):
    q_normed = rms_scale(q_latent.astype(jnp.float32), q_latent_gain).astype(jnp.bfloat16)
    kv_normed = rms_scale(kv_latent.astype(jnp.float32), kv_latent_gain).astype(jnp.bfloat16)
    positions = jnp.arange(TOKENS, dtype=jnp.int32)
    head_q = jnp.moveaxis(w_query.reshape(Q_RANK, HEADS, NOPE_DIM + ROPE_DIM), 1, 0)
    head_k = jnp.moveaxis(w_key.reshape(KV_RANK, HEADS, NOPE_DIM), 1, 0)
    head_v = jnp.moveaxis(w_value.reshape(KV_RANK, HEADS, VALUE_DIM), 1, 0)
    shared = rope_key.astype(jnp.float32)
    score_scale = (NOPE_DIM + ROPE_DIM) ** (-0.5)

    def one_head(head_weights):
        weight_q, weight_k, weight_v = head_weights
        queries = rms_scale(jnp.dot(q_normed, weight_q, preferred_element_type=jnp.float32), query_gain)
        queries = jnp.concatenate([queries[:, :NOPE_DIM], rotate(queries[:, NOPE_DIM:], positions)], axis=-1).astype(jnp.bfloat16)
        keys = jnp.concatenate([jnp.dot(kv_normed, weight_k, preferred_element_type=jnp.float32), shared], axis=-1)
        keys = rms_scale(keys, key_gain)
        keys = jnp.concatenate([keys[:, :NOPE_DIM], rotate(keys[:, NOPE_DIM:], positions)], axis=-1).astype(jnp.bfloat16)
        values = jnp.dot(kv_normed, weight_v, preferred_element_type=jnp.float32).astype(jnp.bfloat16)

        def query_block(row_data):
            scores = jnp.dot(row_data, keys.T, preferred_element_type=jnp.float32) * score_scale
            probs_f = jnp.exp(scores)
            totals = lax.optimization_barrier(jnp.sum(probs_f, axis=-1, keepdims=True))
            mixed = jnp.dot(probs_f.astype(jnp.bfloat16), values, preferred_element_type=jnp.float32)
            return (mixed / totals).astype(jnp.bfloat16)
        blocks = lax.map(query_block, queries.reshape(N_EP, ROWS, NOPE_DIM + ROPE_DIM))
        return blocks.reshape(TOKENS, VALUE_DIM)
    head_out = lax.map(one_head, (head_q, head_k, head_v))
    per_group = HEADS // N_TP
    mixed_sum = jnp.zeros((TOKENS, MODEL_DIM), jnp.float32)
    for group_index in range(N_TP):
        group_heads = jnp.moveaxis(head_out[group_index * per_group:(group_index + 1) * per_group], 0, 1)
        group_heads = group_heads.reshape(TOKENS, per_group * VALUE_DIM)
        rows_w = w_mix[group_index * per_group * VALUE_DIM:(group_index + 1) * per_group * VALUE_DIM]
        partial_value = lax.optimization_barrier(jnp.dot(group_heads, rows_w, preferred_element_type=jnp.float32).astype(jnp.bfloat16))
        mixed_sum = mixed_sum + partial_value.astype(jnp.float32)
    mix_out = mixed_sum.astype(jnp.bfloat16)
    b_normed = rms_scale(tokens_b.astype(jnp.float32), norm_gain).astype(jnp.bfloat16)
    flat_ids = expert_ids.reshape(-1)
    flat_weights = route_weights.reshape(-1)
    max_rows = N_EP * N_TP * CAP_SLOTS
    hidden_dim = FF_DIM // N_TP

    def one_expert(totals, expert):
        chosen = flat_ids == expert
        picked = jnp.nonzero(chosen, size=max_rows, fill_value=0)[0]
        is_live = jnp.arange(max_rows) < jnp.sum(chosen.astype(jnp.int32))
        owners = picked // TOP_K
        row_data = b_normed[owners]
        gate_pre = jnp.dot(row_data, w_gate[expert], preferred_element_type=jnp.float32)
        up_pre = jnp.dot(row_data, w_up[expert], preferred_element_type=jnp.float32)
        hidden = (jax.nn.silu(gate_pre) * up_pre).astype(jnp.bfloat16)
        partial_value = jnp.einsum('rtf,tfd->trd', hidden.reshape(max_rows, N_TP, hidden_dim).astype(jnp.float32), w_down[expert].reshape(N_TP, hidden_dim, MODEL_DIM).astype(jnp.float32))
        rounded = lax.optimization_barrier(partial_value.astype(jnp.bfloat16))
        result = lax.optimization_barrier(jnp.sum(rounded.astype(jnp.float32), axis=0)).astype(jnp.bfloat16)
        scaled = jnp.where(is_live, flat_weights[picked], 0.0)
        return (totals.at[owners].add(scaled[:, None] * result.astype(jnp.float32)), None)
    totals, _ = lax.scan(one_expert, jnp.zeros((TOKENS, MODEL_DIM), jnp.float32), jnp.arange(EXPERTS, dtype=jnp.int32))
    return (mix_out, totals.astype(jnp.bfloat16))
```

```python
import jax
import jax.numpy as jnp
from jax import lax
from jax.experimental import pallas as pl
from jax.experimental.pallas import tpu as pltpu
from jax.sharding import PartitionSpec as P


NOPE_DIM = 128
ROPE_DIM = 64
VALUE_DIM = 128
HEAD_DIM = NOPE_DIM + ROPE_DIM
EXPERTS = 32
TOP_K = 2
CAP = 4
SIDE = 4
EPSILON = 1e-06
THETA = 10000.0
LANES = 128
LOG2E = 1.4426950408889634

BF16 = jnp.bfloat16
F32 = jnp.float32


def params(mib=56):
    return pltpu.CompilerParams(vmem_limit_bytes=mib * 1024 * 1024)


def rms(values, gains):
    return values * lax.rsqrt(jnp.mean(values * values, axis=-1, keepdims=True) + EPSILON) * gains


def latent_body(q_ref, kv_ref, rope_ref, qg_ref, kvg_ref, out_ref):
    rows = q_ref.shape[0]
    q = rms(q_ref[...].astype(F32), qg_ref[...]).astype(BF16)
    kv = rms(kv_ref[...].astype(F32), kvg_ref[...]).astype(BF16)
    rope = rope_ref[...]
    parts = [p[:, j : j + LANES] for p in (q, kv) for j in range(0, p.shape[1], LANES)]
    parts.append(jnp.concatenate([rope, jnp.zeros_like(rope)], axis=1))
    for n, part in enumerate(parts):
        out_ref[n * rows : (n + 1) * rows, :] = part


def square(row):
    return jnp.broadcast_to(row, (row.shape[1], row.shape[1]))


def slots_of(rows, as_rows):
    count = rows.shape[1]
    line = lax.broadcasted_iota(jnp.int32, (count, count), 0)
    lane = lax.broadcasted_iota(jnp.int32, (count, count), 1)
    ids = [square(rows[k : k + 1, :].astype(F32)) for k in range(TOP_K)]
    outs = []
    for k in range(TOP_K):
        if as_rows:
            same = sum(jnp.where((p.T == ids[k]) & (line < lane), 1.0, 0.0) for p in ids)
            picked = ids[k][:1, :] * CAP + jnp.sum(same, axis=0, keepdims=True)
        else:
            mine = ids[k].T
            same = sum(jnp.where((p == mine) & (lane < line), 1.0, 0.0) for p in ids)
            picked = mine[:, :1] * CAP + jnp.sum(same, axis=1, keepdims=True)
        outs.append(picked.astype(jnp.int32))
    return outs


def dispatch_body(tok_ref, gain_ref, rows_ref, out_ref):
    normed = rms(tok_ref[...].astype(F32), gain_ref[...]).astype(BF16)
    first, second = slots_of(rows_ref[...], True)
    shape = (out_ref.shape[0], normed.shape[0])
    slot = lax.broadcasted_iota(jnp.int32, shape, 0)
    hot = jnp.where((slot == first) | (slot == second), 1.0, 0.0).astype(BF16)
    out_ref[...] = jnp.dot(hot, normed, preferred_element_type=F32).astype(BF16)


def collect_body(back_ref, rows_ref, weight_ref, out_ref):
    first, second = slots_of(rows_ref[...], False)
    count = out_ref.shape[0]
    slot = lax.broadcasted_iota(jnp.int32, (count, back_ref.shape[0]), 1)
    weights = [square(weight_ref[k : k + 1, :]).T[:, :1] for k in range(TOP_K)]
    mixed = jnp.where(slot == first, weights[0], 0.0) + jnp.where(slot == second, weights[1], 0.0)
    high = mixed.astype(BF16)
    rest = mixed - high.astype(F32)
    low = rest.astype(BF16)
    last = (rest - low.astype(F32)).astype(BF16)
    back = back_ref[...]
    total = jnp.dot(high, back, preferred_element_type=F32)
    total += jnp.dot(low, back, preferred_element_type=F32)
    total += jnp.dot(last, back, preferred_element_type=F32)
    out_ref[...] = total.astype(BF16)


def turned(values, cosine, sine):
    half = values.shape[-1] // 2
    swapped = jnp.concatenate([values[:, half:], values[:, :half]], axis=1)
    return values * cosine + swapped * sine


def project_body(
    lat_ref, wq_ref, wk_ref, wv_ref, qg_ref, kg_ref, cos_ref, sin_ref, q_ref, kv_ref, lat_q, lat_kv
):
    groups, height, _ = lat_ref.shape
    q_parts = lat_q.shape[1] // LANES
    kv_parts = lat_kv.shape[1] // LANES
    own = height // (q_parts + kv_parts + 1)
    half = groups * own // 2
    for j in range(q_parts + kv_parts):
        piece = lat_ref[:, j * own : (j + 1) * own, :].reshape(2 * half, LANES)
        dst, col = (lat_q, j) if j < q_parts else (lat_kv, j - q_parts)
        dst[:, col * LANES : (col + 1) * LANES] = piece
    rope = lat_ref[:, (q_parts + kv_parts) * own :, :].reshape(2 * half, LANES)[:, :ROPE_DIM]
    rope = rope.astype(F32)
    cosine, sine = cos_ref[...], sin_ref[...]
    queries = jnp.dot(lat_q[...], wq_ref[...], preferred_element_type=F32)
    scale = HEAD_DIM**-0.5 * LOG2E
    queries = rms(queries, qg_ref[...] * scale)
    q_ref[: 2 * half, :] = queries[:, :NOPE_DIM].astype(BF16)
    q_rope = turned(queries[:, NOPE_DIM:], cosine, sine).astype(BF16)
    q_ref[2 * half :, :] = jnp.concatenate([q_rope[:half], q_rope[half:]], axis=1)
    latent = lat_kv[...]
    keys = jnp.dot(latent, wk_ref[...], preferred_element_type=F32)
    square = jnp.sum(keys * keys, axis=-1, keepdims=True) + jnp.sum(
        rope * rope, axis=-1, keepdims=True
    )
    factor = lax.rsqrt(square / HEAD_DIM + EPSILON)
    gains = kg_ref[...]
    kv_ref[: 2 * half, :] = (keys * factor * gains[:, :NOPE_DIM]).astype(BF16)
    kv_ref[2 * half : 4 * half, :] = jnp.dot(
        latent, wv_ref[...], preferred_element_type=F32
    ).astype(BF16)
    k_rope = turned(rope * factor * gains[:, NOPE_DIM:], cosine, sine).astype(BF16)
    kv_ref[4 * half :, :] = jnp.concatenate([k_rope[:half], k_rope[half:]], axis=1)


def attend_body(*refs):
    q_refs, kv_refs, out_refs = refs[:SIDE], refs[SIDE : 2 * SIDE], refs[2 * SIDE : 3 * SIDE]
    qs, ks, vs, acc_ref = refs[3 * SIDE :]
    rows = qs.shape[0] // SIDE
    half = rows // 2
    zero = jnp.zeros((half, ROPE_DIM), BF16)
    ones = jnp.ones((rows, LANES), BF16)
    for b in range(SIDE):
        at = b * rows
        for src, dst, off in ((q_refs[b], qs, rows), (kv_refs[b], ks, 2 * rows)):
            dst[at : at + rows, :NOPE_DIM] = src[:rows, :]
            packed = src[off : off + half, :]
            dst[at : at + half, NOPE_DIM:] = jnp.concatenate([packed[:, :ROPE_DIM], zero], axis=1)
            dst[at + half : at + rows, NOPE_DIM:] = jnp.concatenate(
                [packed[:, ROPE_DIM:], zero], axis=1
            )
        vs[at : at + rows, :VALUE_DIM] = kv_refs[b][rows : 2 * rows, :]
        vs[at : at + rows, VALUE_DIM:] = ones

    def block(i, carry):
        here = pl.ds(pl.multiple_of(i * rows, rows), rows)
        q = qs[here, :]
        acc = None
        for b in range(SIDE):
            there = slice(b * rows, (b + 1) * rows)
            scores = lax.dot_general(
                q, ks[there, :], (((1,), (1,)), ((), ())), preferred_element_type=F32
            )
            probs = jnp.exp2(scores).astype(BF16)
            term = jnp.dot(probs, vs[there, :], preferred_element_type=F32)
            acc = term if acc is None else acc + term
        acc_ref[here, :] = acc
        return carry

    lax.fori_loop(0, SIDE, block, 0)
    for b in range(SIDE):
        at = b * rows
        out_refs[b][:rows, :] = acc_ref[at : at + rows, :VALUE_DIM].astype(BF16)
        for j in range(rows // LANES):
            total = acc_ref[at + j * LANES : at + (j + 1) * LANES, VALUE_DIM:].T[0:1, :]
            high = total.astype(BF16)
            low = (total - high.astype(F32)).astype(BF16)
            out_refs[b][rows + j : rows + j + 1, :] = high
            out_refs[b][rows + 8 + j : rows + 8 + j + 1, :] = low


def mix_body(*refs):
    parts = refs[:SIDE]
    w_ref, _, out_ref, head_ref, term_ref, sems = refs[SIDE:]
    rows = head_ref.shape[0]
    owners, span, _ = out_ref.shape
    own = rows // owners
    count = rows // LANES
    total = sum(p[rows : rows + 8, :].astype(F32) + p[rows + 8 : rows + 16, :].astype(F32) for p in parts)
    inverse = 1.0 / total
    for j in range(count):
        there = slice(j * LANES, (j + 1) * LANES)
        scale = jnp.broadcast_to(inverse[j : j + 1, :], (LANES, LANES)).T
        head = sum(p[there, :].astype(F32) for p in parts)
        head_ref[there, :] = (head * scale).astype(BF16)
    copies = []
    step = owners // 4
    for c in range(4):
        there = slice(c * step * own, (c + 1) * step * own)
        term_ref[there, :] = jnp.dot(
            head_ref[there, :], w_ref[...], preferred_element_type=F32
        ).astype(BF16)
        for i in range(c * step, (c + 1) * step):
            copy = pltpu.make_async_copy(
                term_ref.at[pl.ds(i * own, own), :],
                out_ref.at[i, pl.ds(span - own, own), :],
                sems.at[i],
            )
            copy.start()
            copies.append(copy)
    for copy in copies:
        copy.wait()


def expert_body(x_ref, gate_ref, up_ref, down_ref, out_ref):
    groups, _, rows, width = x_ref.shape
    x = x_ref[...].reshape(groups * rows, width)
    gate = jnp.dot(x, gate_ref[0], preferred_element_type=F32)
    up = jnp.dot(x, up_ref[0], preferred_element_type=F32)
    hidden = (gate / (1.0 + jnp.exp(-gate)) * up).astype(BF16)
    out = jnp.dot(hidden, down_ref[0], preferred_element_type=F32).astype(BF16)
    out_ref[...] = out.reshape(groups, rows, width)


def shift(axis_x, axis_y):
    return [
        (y * SIDE + x, ((y + axis_y) % SIDE) * SIDE + (x + axis_x) % SIDE)
        for y in range(SIDE)
        for x in range(SIDE)
    ]


def on_device(
    q_latent,
    kv_latent,
    rope_key,
    q_latent_gain,
    kv_latent_gain,
    w_query,
    w_key,
    w_value,
    query_gain,
    key_gain,
    w_mix,
    tokens_b,
    norm_gain,
    expert_ids,
    route_weights,
    w_gate,
    w_up,
    w_down,
):
    tp_count = lax.axis_size("tp")
    ep_count = lax.axis_size("ep")
    own = q_latent.shape[0]
    rows = own * tp_count
    width = tokens_b.shape[1]
    experts_dev = w_gate.shape[0]
    slots = EXPERTS * CAP

    height = own * ((q_latent.shape[1] + kv_latent.shape[1]) // LANES + 1)
    latent = pl.pallas_call(
        latent_body,
        out_shape=jax.ShapeDtypeStruct((height, LANES), BF16),
        compiler_params=params(),
        name="latents",
    )(q_latent, kv_latent, rope_key, q_latent_gain[None], kv_latent_gain[None])

    latent, tokens_b = lax.optimization_barrier((latent, tokens_b))
    id_rows = expert_ids.T
    outgoing = pl.pallas_call(
        dispatch_body,
        out_shape=jax.ShapeDtypeStruct((slots, width), BF16),
        compiler_params=params(),
        name="dispatch",
    )(tokens_b, norm_gain[None], id_rows)

    latents = lax.all_gather(latent, "tp", axis=0)

    arrived = lax.all_to_all(outgoing.reshape(ep_count, slots // ep_count, width), "ep", 0, 0)
    arrived = arrived.reshape(slots, width)
    at = jnp.arange(slots, dtype=jnp.int32)
    moved = (at % (slots // experts_dev)) // CAP * (experts_dev * CAP) + at // (
        slots // experts_dev
    ) * CAP + at % CAP
    turn = (moved[:, None] == at[None, :]).astype(BF16)
    grouped = jnp.dot(turn, arrived, preferred_element_type=F32).astype(BF16)
    everyone = lax.all_gather(grouped, "tp", axis=0, tiled=True)
    everyone = everyone.reshape(tp_count, experts_dev, slots // experts_dev, width)

    positions = lax.axis_index("ep") * rows + jnp.arange(rows, dtype=jnp.int32)
    inverse = THETA ** (-jnp.arange(0, ROPE_DIM, 2, dtype=F32) / ROPE_DIM)
    angles = positions.astype(F32)[:, None] * inverse[None, :]
    cosine, sine = jnp.cos(angles), jnp.sin(angles)
    cosine = jnp.concatenate([cosine, cosine], axis=1)
    sine = jnp.concatenate([-sine, sine], axis=1)

    q_own, kv_own = pl.pallas_call(
        project_body,
        out_shape=(
            jax.ShapeDtypeStruct((rows + rows // 2, LANES), BF16),
            jax.ShapeDtypeStruct((2 * rows + rows // 2, LANES), BF16),
        ),
        scratch_shapes=[
            pltpu.VMEM((rows, q_latent.shape[1]), BF16),
            pltpu.VMEM((rows, kv_latent.shape[1]), BF16),
        ],
        compiler_params=params(),
        name="project",
    )(latents, w_query, w_key, w_value, query_gain[None], key_gain[None], cosine, sine)

    kv_all = [kv_own] + [lax.ppermute(kv_own, "ep", shift(d, 0)) for d in (1, 3, 2)]
    q_all = [q_own] + [lax.ppermute(q_own, "ep", shift(0, d)) for d in (1, 3, 2)]
    partial = pl.pallas_call(
        attend_body,
        out_shape=[jax.ShapeDtypeStruct((rows + 16, LANES), BF16)] * SIDE,
        scratch_shapes=[pltpu.VMEM((SIDE * rows, 2 * LANES), BF16)] * 3
        + [pltpu.VMEM((SIDE * rows, 2 * LANES), F32)],
        compiler_params=params(),
        name="attend",
    )(*q_all, *kv_all)
    parts = [partial[0]] + [
        lax.ppermute(p, "ep", shift(0, -d)) for p, d in zip(partial[1:], (1, 3, 2))
    ]

    span = slots + own
    share = slots // experts_dev
    step = tp_count // 2
    hidden = w_gate.shape[2]
    terms = pl.pallas_call(
        expert_body,
        out_shape=jax.ShapeDtypeStruct((tp_count, span, width), BF16),
        grid=(experts_dev, tp_count // step),
        in_specs=[
            pl.BlockSpec((step, 1, share, width), lambda x, j: (j, x, 0, 0)),
            pl.BlockSpec((1, width, hidden), lambda x, j: (x, 0, 0)),
            pl.BlockSpec((1, width, hidden), lambda x, j: (x, 0, 0)),
            pl.BlockSpec((1, hidden, width), lambda x, j: (x, 0, 0)),
        ],
        out_specs=pl.BlockSpec((step, share, width), lambda x, j: (j, x, 0)),
        compiler_params=params(),
        name="experts",
    )(everyone, w_gate, w_up, w_down)

    terms = pl.pallas_call(
        mix_body,
        out_shape=jax.ShapeDtypeStruct((tp_count, span, width), BF16),
        in_specs=[pl.BlockSpec(memory_space=pltpu.VMEM)] * (SIDE + 1)
        + [pl.BlockSpec(memory_space=pl.ANY)],
        out_specs=pl.BlockSpec(memory_space=pl.ANY),
        scratch_shapes=[
            pltpu.VMEM((rows, VALUE_DIM), BF16),
            pltpu.VMEM((rows, width), BF16),
            pltpu.SemaphoreType.DMA((tp_count,)),
        ],
        input_output_aliases={SIDE + 1: 0},
        compiler_params=params(),
        name="mix",
    )(*parts, w_mix, terms)

    summed = lax.psum_scatter(
        terms.reshape(tp_count * span, width), "tp", scatter_dimension=0, tiled=True
    )
    mix_out = summed[slots:]
    done = jnp.dot(turn.T, summed[:slots], preferred_element_type=F32).astype(BF16)
    returned = lax.all_to_all(done.reshape(ep_count, slots // ep_count, width), "ep", 0, 0)
    expert_out = pl.pallas_call(
        collect_body,
        out_shape=jax.ShapeDtypeStruct((own, width), BF16),
        compiler_params=params(),
        name="collect",
    )(returned.reshape(slots, width), id_rows, route_weights.T)
    return (mix_out, expert_out)


def solution(mesh):
    in_specs = (
        P(("ep", "tp"), None),
        P(("ep", "tp"), None),
        P(("ep", "tp"), None),
        P(),
        P(),
        P(None, "tp"),
        P(None, "tp"),
        P(None, "tp"),
        P(),
        P(),
        P("tp", None),
        P(("ep", "tp"), None),
        P(),
        P(("ep", "tp"), None),
        P(("ep", "tp"), None),
        P("ep", None, "tp"),
        P("ep", None, "tp"),
        P("ep", "tp", None),
    )
    out_specs = (P(("ep", "tp"), None), P(("ep", "tp"), None))

    return jax.shard_map(
        on_device, mesh=mesh, in_specs=in_specs, out_specs=out_specs, check_vma=False
    )
```

```python
import jax
import jax.numpy as jnp
from jax import lax
from jax.experimental import pallas as pl
from jax.experimental.pallas import tpu as pltpu
from jax.sharding import PartitionSpec as P


NOPE_DIM = 128
ROPE_DIM = 64
VALUE_DIM = 128
HEAD_DIM = NOPE_DIM + ROPE_DIM
EXPERTS = 32
TOP_K = 2
CAP = 4
SIDE = 4
EPSILON = 1e-06
THETA = 10000.0
LANES = 128
LOG2E = 1.4426950408889634


BF16 = jnp.bfloat16
F32 = jnp.float32


def params(mib=56):
    return pltpu.CompilerParams(vmem_limit_bytes=mib * 1024 * 1024)


def rms(values, gains):
    return values * lax.rsqrt(jnp.mean(values * values, axis=-1, keepdims=True) + EPSILON) * gains


def latent_body(q_ref, kv_ref, rope_ref, qg_ref, kvg_ref, out_ref):
    rows = q_ref.shape[0]
    q = rms(q_ref[...].astype(F32), qg_ref[...]).astype(BF16)
    kv = rms(kv_ref[...].astype(F32), kvg_ref[...]).astype(BF16)
    rope = rope_ref[...]
    parts = [p[:, j : j + LANES] for p in (q, kv) for j in range(0, p.shape[1], LANES)]
    parts.append(jnp.concatenate([rope, jnp.zeros_like(rope)], axis=1))
    for n, part in enumerate(parts):
        out_ref[n * rows : (n + 1) * rows, :] = part


def square(row):
    return jnp.broadcast_to(row, (row.shape[1], row.shape[1]))


def slots_of(rows, as_rows):
    count = rows.shape[1]
    line = lax.broadcasted_iota(jnp.int32, (count, count), 0)
    lane = lax.broadcasted_iota(jnp.int32, (count, count), 1)
    ids = [square(rows[k : k + 1, :].astype(F32)) for k in range(TOP_K)]
    outs = []
    for k in range(TOP_K):
        if as_rows:
            same = sum(jnp.where((p.T == ids[k]) & (line < lane), 1.0, 0.0) for p in ids)
            picked = ids[k][:1, :] * CAP + jnp.sum(same, axis=0, keepdims=True)
        else:
            mine = ids[k].T
            same = sum(jnp.where((p == mine) & (lane < line), 1.0, 0.0) for p in ids)
            picked = mine[:, :1] * CAP + jnp.sum(same, axis=1, keepdims=True)
        outs.append(picked.astype(jnp.int32))
    return outs


def dispatch_body(tok_ref, gain_ref, rows_ref, out_ref):
    normed = rms(tok_ref[...].astype(F32), gain_ref[...]).astype(BF16)
    first, second = slots_of(rows_ref[...], True)
    shape = (out_ref.shape[0], normed.shape[0])
    slot = lax.broadcasted_iota(jnp.int32, shape, 0)
    hot = jnp.where((slot == first) | (slot == second), 1.0, 0.0).astype(BF16)
    out_ref[...] = jnp.dot(hot, normed, preferred_element_type=F32).astype(BF16)


def collect_body(back_ref, rows_ref, weight_ref, out_ref):
    first, second = slots_of(rows_ref[...], False)
    count = out_ref.shape[0]
    slot = lax.broadcasted_iota(jnp.int32, (count, back_ref.shape[0]), 1)
    weights = [square(weight_ref[k : k + 1, :]).T[:, :1] for k in range(TOP_K)]
    mixed = jnp.where(slot == first, weights[0], 0.0) + jnp.where(slot == second, weights[1], 0.0)
    high = mixed.astype(BF16)
    rest = mixed - high.astype(F32)
    low = rest.astype(BF16)
    last = (rest - low.astype(F32)).astype(BF16)
    back = back_ref[...]
    total = jnp.dot(high, back, preferred_element_type=F32)
    total += jnp.dot(low, back, preferred_element_type=F32)
    total += jnp.dot(last, back, preferred_element_type=F32)
    out_ref[...] = total.astype(BF16)


def turned(values, cosine, sine):
    half = values.shape[-1] // 2
    swapped = jnp.concatenate([values[:, half:], values[:, :half]], axis=1)
    return values * cosine + swapped * sine


def project_body(
    mine_ref, other_ref, wq_ref, wk_ref, wv_ref, qg_ref, kg_ref, cos_ref, sin_ref,
    q_ref, kv_ref, lat_q, lat_kv,
):
    groups, height, _ = mine_ref.shape
    q_parts = lat_q.shape[1] // LANES
    kv_parts = lat_kv.shape[1] // LANES
    own = height // (q_parts + kv_parts + 1)
    half = groups * own
    ropes = []
    for n, src in enumerate((mine_ref, other_ref)):
        for j in range(q_parts + kv_parts):
            piece = src[:, j * own : (j + 1) * own, :].reshape(half, LANES)
            dst, col = (lat_q, j) if j < q_parts else (lat_kv, j - q_parts)
            dst[n * half : (n + 1) * half, col * LANES : (col + 1) * LANES] = piece
        ropes.append(src[:, (q_parts + kv_parts) * own :, :].reshape(half, LANES)[:, :ROPE_DIM])
    rope = jnp.concatenate(ropes, axis=0).astype(F32)
    cosine, sine = cos_ref[...], sin_ref[...]
    queries = jnp.dot(lat_q[...], wq_ref[...], preferred_element_type=F32)
    scale = HEAD_DIM**-0.5 * LOG2E
    queries = rms(queries, qg_ref[...] * scale)
    q_ref[: 2 * half, :] = queries[:, :NOPE_DIM].astype(BF16)
    q_rope = turned(queries[:, NOPE_DIM:], cosine, sine).astype(BF16)
    q_ref[2 * half :, :] = jnp.concatenate([q_rope[:half], q_rope[half:]], axis=1)
    latent = lat_kv[...]
    keys = jnp.dot(latent, wk_ref[...], preferred_element_type=F32)
    square = jnp.sum(keys * keys, axis=-1, keepdims=True) + jnp.sum(
        rope * rope, axis=-1, keepdims=True
    )
    factor = lax.rsqrt(square / HEAD_DIM + EPSILON)
    gains = kg_ref[...]
    kv_ref[: 2 * half, :] = (keys * factor * gains[:, :NOPE_DIM]).astype(BF16)
    kv_ref[2 * half : 4 * half, :] = jnp.dot(
        latent, wv_ref[...], preferred_element_type=F32
    ).astype(BF16)
    k_rope = turned(rope * factor * gains[:, NOPE_DIM:], cosine, sine).astype(BF16)
    kv_ref[4 * half :, :] = jnp.concatenate([k_rope[:half], k_rope[half:]], axis=1)


def attend(q_refs, kv_refs, start, finish, qs, ks, vs):
    rows = qs.shape[0] // SIDE
    half = rows // 2
    zero = jnp.zeros((half, ROPE_DIM), BF16)
    ones = jnp.ones((rows, LANES), BF16)
    staged = [(r, qs, b, rows) for b, r in enumerate(q_refs)]
    staged += [(r, ks, b, 2 * rows) for b, r in enumerate(kv_refs)]
    for src, dst, b, off in staged:
        at = b * rows
        dst[at : at + rows, :NOPE_DIM] = src[:rows, :]
        packed = src[off : off + half, :]
        dst[at : at + half, NOPE_DIM:] = jnp.concatenate([packed[:, :ROPE_DIM], zero], axis=1)
        dst[at + half : at + rows, NOPE_DIM:] = jnp.concatenate([packed[:, ROPE_DIM:], zero], axis=1)
    for b, src in enumerate(kv_refs):
        vs[b * rows : (b + 1) * rows, :VALUE_DIM] = src[rows : 2 * rows, :]
        vs[b * rows : (b + 1) * rows, VALUE_DIM:] = ones

    def block(i, carry):
        here = pl.ds(pl.multiple_of(i * rows, rows), rows)
        q = qs[here, :]
        acc = start(here)
        for b in range(len(kv_refs)):
            there = slice(b * rows, (b + 1) * rows)
            scores = lax.dot_general(
                q, ks[there, :], (((1,), (1,)), ((), ())), preferred_element_type=F32
            )
            probs = jnp.exp2(scores).astype(BF16)
            term = jnp.dot(probs, vs[there, :], preferred_element_type=F32)
            acc = term if acc is None else acc + term
        finish(here, acc)
        return carry

    lax.fori_loop(0, SIDE, block, 0)


def near_body(*refs):
    q_refs, kv_refs, (acc_ref, qs, ks, vs) = refs[:SIDE], refs[SIDE:-4], refs[-4:]

    def finish(here, acc):
        acc_ref[here, :] = acc

    attend(q_refs, kv_refs, lambda here: None, finish, qs, ks, vs)


def far_body(*refs):
    q_refs, (kv_ref, in_ref), rest = refs[:SIDE], refs[SIDE : SIDE + 2], refs[SIDE + 2 :]
    out_refs, (qs, ks, vs, acc_ref) = rest[:SIDE], rest[SIDE:]
    rows = qs.shape[0] // SIDE

    def finish(here, acc):
        acc_ref[here, :] = acc

    attend(q_refs, (kv_ref,), lambda here: in_ref[here, :], finish, qs, ks, vs)
    for b in range(SIDE):
        at = b * rows
        out_refs[b][:rows, :] = acc_ref[at : at + rows, :VALUE_DIM].astype(BF16)
        for j in range(rows // LANES):
            total = acc_ref[at + j * LANES : at + (j + 1) * LANES, VALUE_DIM:].T[0:1, :]
            high = total.astype(BF16)
            low = (total - high.astype(F32)).astype(BF16)
            out_refs[b][rows + j : rows + j + 1, :] = high
            out_refs[b][rows + 8 + j : rows + 8 + j + 1, :] = low


def stack_body(*refs):
    for n, ref in enumerate(refs[:-1]):
        refs[-1][n, :, :] = ref[...]


def join_body(*refs):
    parts, outs = refs[:SIDE], refs[SIDE:]
    half = outs[0].shape[0]
    rows = 2 * half
    total = sum(
        p[rows : rows + 8, :].astype(F32) + p[rows + 8 : rows + 16, :].astype(F32) for p in parts
    )
    inverse = 1.0 / total
    for j in range(rows // LANES):
        there = slice(j * LANES, (j + 1) * LANES)
        scale = jnp.broadcast_to(inverse[j : j + 1, :], (LANES, LANES)).T
        head = sum(p[there, :].astype(F32) for p in parts)
        at = j * LANES % half
        outs[j * LANES // half][at : at + LANES, :] = (head * scale).astype(BF16)


def mix_body(chip_ref, own_ref, twin_ref, w_own_ref, w_twin_ref, _, out_ref, term_ref, sems):
    owners, span, _ = out_ref.shape
    each = own_ref.shape[0] // owners
    step = owners // 2
    copies = []
    for c in range(2):
        there = slice(c * step * each, (c + 1) * step * each)
        term = jnp.dot(own_ref[there, :], w_own_ref[...], preferred_element_type=F32)
        term += jnp.dot(twin_ref[there, :], w_twin_ref[...], preferred_element_type=F32)
        term_ref[there, :] = term.astype(BF16)
        for i in range(c * step, (c + 1) * step):
            copy = pltpu.make_async_copy(
                term_ref.at[pl.ds(i * each, each), :],
                out_ref.at[(chip_ref[0] + owners - i) % owners, pl.ds(span - each, each), :],
                sems.at[i],
            )
            copy.start()
            copies.append(copy)
    for copy in copies:
        copy.wait()


def expert_body(core_ref, x_ref, *refs):
    del core_ref
    sets, out_ref = (refs[:3], refs[3:6]), refs[6]
    groups, rows, width = x_ref.shape
    x = x_ref[...].reshape(groups * rows, width)
    out = None
    for gate_ref, up_ref, down_ref in sets:
        gate = jnp.dot(x, gate_ref[...].reshape(width, -1), preferred_element_type=F32)
        up = jnp.dot(x, up_ref[...].reshape(width, -1), preferred_element_type=F32)
        hidden = (gate / (1.0 + jnp.exp(-gate)) * up).astype(BF16)
        term = jnp.dot(hidden, down_ref[...].reshape(-1, width), preferred_element_type=F32)
        out = term if out is None else out + term
    out_ref[...] = out.astype(BF16).reshape(groups, rows, width)


def shift(axis_x, axis_y):
    return [
        (y * SIDE + x, ((y + axis_y) % SIDE) * SIDE + (x + axis_x) % SIDE)
        for y in range(SIDE)
        for x in range(SIDE)
    ]


def on_device(
    q_latent,
    kv_latent,
    rope_key,
    q_latent_gain,
    kv_latent_gain,
    w_query,
    w_key,
    w_value,
    query_gain,
    key_gain,
    w_mix,
    tokens_b,
    norm_gain,
    expert_ids,
    route_weights,
    w_gate,
    w_up,
    w_down,
):
    tp_count = lax.axis_size("tp")
    ep_count = lax.axis_size("ep")
    chips = tp_count // 2
    own = q_latent.shape[0]
    rows = own * tp_count
    half = rows // 2
    width = tokens_b.shape[1]
    slots = EXPERTS * CAP
    tp_at = lax.axis_index("tp")
    core, chip = tp_at % 2, tp_at // 2
    same_core = [[z * 2 + c for z in range(chips)] for c in range(2)]
    plane = [
        [e * tp_count + z * 2 + c for e in range(ep_count) for c in range(2)] for z in range(chips)
    ]
    swap = [(i, i ^ 1) for i in range(tp_count)]

    height = own * ((q_latent.shape[1] + kv_latent.shape[1]) // LANES + 1)
    latent = pl.pallas_call(
        latent_body,
        out_shape=jax.ShapeDtypeStruct((height, LANES), BF16),
        compiler_params=params(),
        name="latents",
    )(q_latent, kv_latent, rope_key, q_latent_gain[None], kv_latent_gain[None])

    id_rows = expert_ids.T
    outgoing = pl.pallas_call(
        dispatch_body,
        out_shape=jax.ShapeDtypeStruct((slots, width), BF16),
        compiler_params=params(),
        name="dispatch",
    )(tokens_b, norm_gain[None], id_rows)

    arrived = lax.all_to_all(
        outgoing.reshape(EXPERTS, CAP, width), ("ep", "tp"), 0, 0, axis_index_groups=plane
    )
    everyone = lax.all_gather(
        arrived.reshape(slots, width), "tp", axis=0, axis_index_groups=same_core
    )

    mine = [latent] + [
        lax.ppermute(latent, "tp", [(i, (i + 2 * k) % tp_count) for i in range(tp_count)])
        for k in range(1, chips)
    ]
    mine = pl.pallas_call(
        stack_body,
        out_shape=jax.ShapeDtypeStruct((chips, height, LANES), BF16),
        compiler_params=params(),
        name="stack",
    )(*mine)
    other = lax.ppermute(mine, "tp", swap)

    block = jnp.arange(rows, dtype=jnp.int32) // own
    side = jnp.where(block < chips, core, 1 - core)
    positions = (
        lax.axis_index("ep") * rows
        + (((chip - block) % chips) * 2 + side) * own
        + jnp.arange(rows, dtype=jnp.int32) % own
    )
    inverse = THETA ** (-jnp.arange(0, ROPE_DIM, 2, dtype=F32) / ROPE_DIM)
    angles = positions.astype(F32)[:, None] * inverse[None, :]
    cosine, sine = jnp.cos(angles), jnp.sin(angles)
    cosine = jnp.concatenate([cosine, cosine], axis=1)
    sine = jnp.concatenate([-sine, sine], axis=1)

    q_own, kv_own = pl.pallas_call(
        project_body,
        out_shape=(
            jax.ShapeDtypeStruct((rows + rows // 2, LANES), BF16),
            jax.ShapeDtypeStruct((2 * rows + rows // 2, LANES), BF16),
        ),
        scratch_shapes=[
            pltpu.VMEM((rows, q_latent.shape[1]), BF16),
            pltpu.VMEM((rows, kv_latent.shape[1]), BF16),
        ],
        compiler_params=params(),
        name="project",
    )(mine, other, w_query, w_key, w_value, query_gain[None], key_gain[None], cosine, sine)

    kv_near = [kv_own] + [lax.ppermute(kv_own, "ep", shift(d, 0)) for d in (1, 3)]
    q_all = [q_own] + [lax.ppermute(q_own, "ep", shift(0, d)) for d in (1, 3, 2)]
    kv_far = lax.ppermute(kv_own, "ep", shift(2, 0))
    wide = 2 * LANES
    acc = pl.pallas_call(
        near_body,
        out_shape=jax.ShapeDtypeStruct((SIDE * rows, wide), F32),
        scratch_shapes=[
            pltpu.VMEM((SIDE * rows, wide), BF16),
            pltpu.VMEM((3 * rows, wide), BF16),
            pltpu.VMEM((3 * rows, wide), BF16),
        ],
        compiler_params=params(),
        name="near",
    )(*q_all, *kv_near)
    partial = pl.pallas_call(
        far_body,
        out_shape=[jax.ShapeDtypeStruct((rows + 16, LANES), BF16)] * SIDE,
        scratch_shapes=[
            pltpu.VMEM((SIDE * rows, wide), BF16),
            pltpu.VMEM((rows, wide), BF16),
            pltpu.VMEM((rows, wide), BF16),
            pltpu.VMEM((SIDE * rows, wide), F32),
        ],
        compiler_params=params(),
        name="far",
    )(*q_all, kv_far, acc)
    parts = [partial[0]] + [
        lax.ppermute(p, "ep", shift(0, -d)) for p, d in zip(partial[1:], (1, 3, 2))
    ]

    twin = [
        lax.ppermute(lax.dynamic_index_in_dim(w, 1 - core, 0, False), "tp", swap)
        for w in (w_gate, w_up, w_down)
    ]
    mix_twin = lax.ppermute(w_mix, "tp", swap)

    span = slots + own
    step = chips // 2
    hidden = w_gate.shape[2]
    terms = pl.pallas_call(
        expert_body,
        out_shape=jax.ShapeDtypeStruct((chips, span, width), BF16),
        grid_spec=pltpu.PrefetchScalarGridSpec(
            num_scalar_prefetch=1,
            grid=(chips // step,),
            in_specs=[
                pl.BlockSpec((step, slots, width), lambda j, c: (j, 0, 0)),
                pl.BlockSpec((1, width, hidden), lambda j, c: (c[0], 0, 0)),
                pl.BlockSpec((1, width, hidden), lambda j, c: (c[0], 0, 0)),
                pl.BlockSpec((1, hidden, width), lambda j, c: (c[0], 0, 0)),
                pl.BlockSpec((width, hidden), lambda j, c: (0, 0)),
                pl.BlockSpec((width, hidden), lambda j, c: (0, 0)),
                pl.BlockSpec((hidden, width), lambda j, c: (0, 0)),
            ],
            out_specs=pl.BlockSpec((step, slots, width), lambda j, c: (j, 0, 0)),
        ),
        compiler_params=params(),
        name="experts",
    )(core.reshape(1), everyone, w_gate, w_up, w_down, *twin)

    own_head, twin_head = pl.pallas_call(
        join_body,
        out_shape=[jax.ShapeDtypeStruct((half, VALUE_DIM), BF16)] * 2,
        compiler_params=params(),
        name="join",
    )(*parts)
    twin_head = lax.ppermute(twin_head, "tp", swap)
    terms = pl.pallas_call(
        mix_body,
        out_shape=jax.ShapeDtypeStruct((chips, span, width), BF16),
        in_specs=[pl.BlockSpec(memory_space=pltpu.SMEM)]
        + [pl.BlockSpec(memory_space=pltpu.VMEM)] * 4
        + [pl.BlockSpec(memory_space=pl.ANY)],
        out_specs=pl.BlockSpec(memory_space=pl.ANY),
        scratch_shapes=[
            pltpu.VMEM((half, width), BF16),
            pltpu.SemaphoreType.DMA((chips,)),
        ],
        input_output_aliases={5: 0},
        compiler_params=params(),
        name="mix",
    )(chip.reshape(1), own_head, twin_head, w_mix, mix_twin, terms)

    summed = lax.psum_scatter(
        terms.reshape(chips * span, width),
        "tp",
        scatter_dimension=0,
        tiled=True,
        axis_index_groups=same_core,
    )
    mix_out = summed[slots:]
    returned = lax.all_to_all(
        summed[:slots].reshape(EXPERTS, CAP, width), ("ep", "tp"), 0, 0, axis_index_groups=plane
    )
    expert_out = pl.pallas_call(
        collect_body,
        out_shape=jax.ShapeDtypeStruct((own, width), BF16),
        compiler_params=params(),
        name="collect",
    )(returned.reshape(slots, width), id_rows, route_weights.T)
    return (mix_out, expert_out)


def solution(mesh):
    in_specs = (
        P(("ep", "tp"), None),
        P(("ep", "tp"), None),
        P(("ep", "tp"), None),
        P(),
        P(),
        P(None, "tp"),
        P(None, "tp"),
        P(None, "tp"),
        P(),
        P(),
        P("tp", None),
        P(("ep", "tp"), None),
        P(),
        P(("ep", "tp"), None),
        P(("ep", "tp"), None),
        P("ep", None, "tp"),
        P("ep", None, "tp"),
        P("ep", "tp", None),
    )
    out_specs = (P(("ep", "tp"), None), P(("ep", "tp"), None))

    return jax.shard_map(
        on_device, mesh=mesh, in_specs=in_specs, out_specs=out_specs, check_vma=False
    )
```

```python
import jax
import jax.numpy as jnp
from jax import lax
from jax.experimental import pallas as pl
from jax.experimental.pallas import tpu as pltpu
from jax.sharding import PartitionSpec as P


NOPE_DIM = 128
ROPE_DIM = 64
VALUE_DIM = 128
HEAD_DIM = NOPE_DIM + ROPE_DIM
EXPERTS = 32
TOP_K = 2
CAP = 4
SIDE = 4
EPSILON = 1e-06
THETA = 10000.0
LANES = 128
LOG2E = 1.4426950408889634


BF16 = jnp.bfloat16
F32 = jnp.float32


def params(mib=56):
    return pltpu.CompilerParams(vmem_limit_bytes=mib * 1024 * 1024)


def rms(values, gains):
    return values * lax.rsqrt(jnp.mean(values * values, axis=-1, keepdims=True) + EPSILON) * gains


def latent_body(q_ref, kv_ref, rope_ref, qg_ref, kvg_ref, out_ref):
    rows = q_ref.shape[0]
    q = rms(q_ref[...].astype(F32), qg_ref[...]).astype(BF16)
    kv = rms(kv_ref[...].astype(F32), kvg_ref[...]).astype(BF16)
    rope = rope_ref[...]
    parts = [p[:, j : j + LANES] for p in (q, kv) for j in range(0, p.shape[1], LANES)]
    parts.append(jnp.concatenate([rope, jnp.zeros_like(rope)], axis=1))
    for n, part in enumerate(parts):
        for peer in range(out_ref.shape[0]):
            out_ref[peer, n * rows : (n + 1) * rows, :] = part


def square(row):
    return jnp.broadcast_to(row, (row.shape[1], row.shape[1]))


def slots_of(rows, as_rows):
    count = rows.shape[1]
    line = lax.broadcasted_iota(jnp.int32, (count, count), 0)
    lane = lax.broadcasted_iota(jnp.int32, (count, count), 1)
    ids = [square(rows[k : k + 1, :].astype(F32)) for k in range(TOP_K)]
    outs = []
    for k in range(TOP_K):
        if as_rows:
            same = sum(jnp.where((p.T == ids[k]) & (line < lane), 1.0, 0.0) for p in ids)
            picked = ids[k][:1, :] * CAP + jnp.sum(same, axis=0, keepdims=True)
        else:
            mine = ids[k].T
            same = sum(jnp.where((p == mine) & (lane < line), 1.0, 0.0) for p in ids)
            picked = mine[:, :1] * CAP + jnp.sum(same, axis=1, keepdims=True)
        outs.append(picked.astype(jnp.int32))
    return outs


def dispatch_body(tok_ref, gain_ref, rows_ref, out_ref):
    normed = rms(tok_ref[...].astype(F32), gain_ref[...]).astype(BF16)
    first, second = slots_of(rows_ref[...], True)
    shape = (out_ref.shape[0], normed.shape[0])
    slot = lax.broadcasted_iota(jnp.int32, shape, 0)
    hot = jnp.where((slot == first) | (slot == second), 1.0, 0.0).astype(BF16)
    out_ref[...] = jnp.dot(hot, normed, preferred_element_type=F32).astype(BF16)


def collect_body(back_ref, rows_ref, weight_ref, out_ref):
    first, second = slots_of(rows_ref[...], False)
    count = out_ref.shape[0]
    slot = lax.broadcasted_iota(jnp.int32, (count, back_ref.shape[0]), 1)
    weights = [square(weight_ref[k : k + 1, :]).T[:, :1] for k in range(TOP_K)]
    mixed = jnp.where(slot == first, weights[0], 0.0) + jnp.where(slot == second, weights[1], 0.0)
    high = mixed.astype(BF16)
    rest = mixed - high.astype(F32)
    low = rest.astype(BF16)
    last = (rest - low.astype(F32)).astype(BF16)
    back = back_ref[...]
    total = jnp.dot(high, back, preferred_element_type=F32)
    total += jnp.dot(low, back, preferred_element_type=F32)
    total += jnp.dot(last, back, preferred_element_type=F32)
    out_ref[...] = total.astype(BF16)


def turned(values, cosine, sine):
    half = values.shape[-1] // 2
    swapped = jnp.concatenate([values[:, half:], values[:, :half]], axis=1)
    return values * cosine + swapped * sine


def project_body(
    mine_ref, other_ref, wq_ref, wk_ref, wv_ref, qg_ref, kg_ref, cos_ref, sin_ref,
    q_ref, kv_ref, lat_q, lat_kv,
):
    groups, height, _ = mine_ref.shape
    q_parts = lat_q.shape[1] // LANES
    kv_parts = lat_kv.shape[1] // LANES
    own = height // (q_parts + kv_parts + 1)
    half = groups * own
    ropes = []
    for n, src in enumerate((mine_ref, other_ref)):
        for j in range(q_parts + kv_parts):
            piece = src[:, j * own : (j + 1) * own, :].reshape(half, LANES)
            dst, col = (lat_q, j) if j < q_parts else (lat_kv, j - q_parts)
            dst[n * half : (n + 1) * half, col * LANES : (col + 1) * LANES] = piece
        ropes.append(src[:, (q_parts + kv_parts) * own :, :].reshape(half, LANES)[:, :ROPE_DIM])
    rope = jnp.concatenate(ropes, axis=0).astype(F32)
    cosine, sine = cos_ref[...], sin_ref[...]
    queries = jnp.dot(lat_q[...], wq_ref[...], preferred_element_type=F32)
    scale = HEAD_DIM**-0.5 * LOG2E
    queries = rms(queries, qg_ref[...] * scale)
    q_ref[: 2 * half, :] = queries[:, :NOPE_DIM].astype(BF16)
    q_rope = turned(queries[:, NOPE_DIM:], cosine, sine).astype(BF16)
    q_ref[2 * half :, :] = jnp.concatenate([q_rope[:half], q_rope[half:]], axis=1)
    latent = lat_kv[...]
    keys = jnp.dot(latent, wk_ref[...], preferred_element_type=F32)
    square = jnp.sum(keys * keys, axis=-1, keepdims=True) + jnp.sum(
        rope * rope, axis=-1, keepdims=True
    )
    factor = lax.rsqrt(square / HEAD_DIM + EPSILON)
    gains = kg_ref[...]
    kv_ref[: 2 * half, :] = (keys * factor * gains[:, :NOPE_DIM]).astype(BF16)
    kv_ref[2 * half : 4 * half, :] = jnp.dot(
        latent, wv_ref[...], preferred_element_type=F32
    ).astype(BF16)
    k_rope = turned(rope * factor * gains[:, NOPE_DIM:], cosine, sine).astype(BF16)
    kv_ref[4 * half :, :] = jnp.concatenate([k_rope[:half], k_rope[half:]], axis=1)


def attend_body(*refs):
    q_refs, kv_refs, out_refs = refs[:SIDE], refs[SIDE : 2 * SIDE], refs[2 * SIDE : 3 * SIDE]
    qs, ks, vs, acc_ref = refs[3 * SIDE :]
    rows = qs.shape[0] // SIDE
    half = rows // 2
    zero = jnp.zeros((half, ROPE_DIM), BF16)
    ones = jnp.ones((rows, LANES), BF16)
    for b in range(SIDE):
        at = b * rows
        for src, dst, off in ((q_refs[b], qs, rows), (kv_refs[b], ks, 2 * rows)):
            dst[at : at + rows, :NOPE_DIM] = src[:rows, :]
            packed = src[off : off + half, :]
            dst[at : at + half, NOPE_DIM:] = jnp.concatenate([packed[:, :ROPE_DIM], zero], axis=1)
            dst[at + half : at + rows, NOPE_DIM:] = jnp.concatenate(
                [packed[:, ROPE_DIM:], zero], axis=1
            )
        vs[at : at + rows, :VALUE_DIM] = kv_refs[b][rows : 2 * rows, :]
        vs[at : at + rows, VALUE_DIM:] = ones

    def block(i, carry):
        here = pl.ds(pl.multiple_of(i * rows, rows), rows)
        q = qs[here, :]
        acc = None
        for b in range(SIDE):
            there = slice(b * rows, (b + 1) * rows)
            scores = lax.dot_general(
                q, ks[there, :], (((1,), (1,)), ((), ())), preferred_element_type=F32
            )
            probs = jnp.exp2(scores).astype(BF16)
            term = jnp.dot(probs, vs[there, :], preferred_element_type=F32)
            acc = term if acc is None else acc + term
        acc_ref[here, :] = acc
        return carry

    lax.fori_loop(0, SIDE, block, 0)
    for b in range(SIDE):
        at = b * rows
        out_refs[b][:rows, :] = acc_ref[at : at + rows, :VALUE_DIM].astype(BF16)
        for j in range(rows // LANES):
            total = acc_ref[at + j * LANES : at + (j + 1) * LANES, VALUE_DIM:].T[0:1, :]
            high = total.astype(BF16)
            low = (total - high.astype(F32)).astype(BF16)
            out_refs[b][rows + j : rows + j + 1, :] = high
            out_refs[b][rows + 8 + j : rows + 8 + j + 1, :] = low


def join_body(*refs):
    parts, outs = refs[:SIDE], refs[SIDE:]
    half = outs[0].shape[0]
    rows = 2 * half
    total = sum(
        p[rows : rows + 8, :].astype(F32) + p[rows + 8 : rows + 16, :].astype(F32) for p in parts
    )
    inverse = 1.0 / total
    for j in range(rows // LANES):
        there = slice(j * LANES, (j + 1) * LANES)
        scale = jnp.broadcast_to(inverse[j : j + 1, :], (LANES, LANES)).T
        head = sum(p[there, :].astype(F32) for p in parts)
        at = j * LANES % half
        outs[j * LANES // half][at : at + LANES, :] = (head * scale).astype(BF16)


def mix_body(own_ref, twin_ref, w_own_ref, w_twin_ref, _, out_ref, term_ref, sems):
    owners, span, _ = out_ref.shape
    each = own_ref.shape[0] // owners
    step = owners // 2
    copies = []
    for c in range(2):
        there = slice(c * step * each, (c + 1) * step * each)
        term = jnp.dot(own_ref[there, :], w_own_ref[...], preferred_element_type=F32)
        term += jnp.dot(twin_ref[there, :], w_twin_ref[...], preferred_element_type=F32)
        term_ref[there, :] = term.astype(BF16)
        for i in range(c * step, (c + 1) * step):
            copy = pltpu.make_async_copy(
                term_ref.at[pl.ds(i * each, each), :],
                out_ref.at[i, pl.ds(span - each, each), :],
                sems.at[i],
            )
            copy.start()
            copies.append(copy)
    for copy in copies:
        copy.wait()


def expert_body(core_ref, x_ref, *refs):
    del core_ref
    sets, out_ref = (refs[:3], refs[3:6]), refs[6]
    groups, rows, width = x_ref.shape
    x = x_ref[...].reshape(groups * rows, width)
    out = None
    for gate_ref, up_ref, down_ref in sets:
        gate = jnp.dot(x, gate_ref[...].reshape(width, -1), preferred_element_type=F32)
        up = jnp.dot(x, up_ref[...].reshape(width, -1), preferred_element_type=F32)
        hidden = (gate / (1.0 + jnp.exp(-gate)) * up).astype(BF16)
        term = jnp.dot(hidden, down_ref[...].reshape(-1, width), preferred_element_type=F32)
        out = term if out is None else out + term
    out_ref[...] = out.astype(BF16).reshape(groups, rows, width)


def shift(axis_x, axis_y):
    return [
        (y * SIDE + x, ((y + axis_y) % SIDE) * SIDE + (x + axis_x) % SIDE)
        for y in range(SIDE)
        for x in range(SIDE)
    ]


def on_device(
    q_latent,
    kv_latent,
    rope_key,
    q_latent_gain,
    kv_latent_gain,
    w_query,
    w_key,
    w_value,
    query_gain,
    key_gain,
    w_mix,
    tokens_b,
    norm_gain,
    expert_ids,
    route_weights,
    w_gate,
    w_up,
    w_down,
):
    tp_count = lax.axis_size("tp")
    ep_count = lax.axis_size("ep")
    chips = tp_count // 2
    own = q_latent.shape[0]
    rows = own * tp_count
    half = rows // 2
    width = tokens_b.shape[1]
    slots = EXPERTS * CAP
    tp_at = lax.axis_index("tp")
    core = tp_at % 2
    same_core = [[z * 2 + c for z in range(chips)] for c in range(2)]
    plane = [
        [e * tp_count + z * 2 + c for e in range(ep_count) for c in range(2)] for z in range(chips)
    ]
    swap = [(i, i ^ 1) for i in range(tp_count)]

    height = own * ((q_latent.shape[1] + kv_latent.shape[1]) // LANES + 1)
    latent = pl.pallas_call(
        latent_body,
        out_shape=jax.ShapeDtypeStruct((chips, height, LANES), BF16),
        compiler_params=params(),
        name="latents",
    )(q_latent, kv_latent, rope_key, q_latent_gain[None], kv_latent_gain[None])

    latent, tokens_b = lax.optimization_barrier((latent, tokens_b))
    id_rows = expert_ids.T
    outgoing = pl.pallas_call(
        dispatch_body,
        out_shape=jax.ShapeDtypeStruct((slots, width), BF16),
        compiler_params=params(),
        name="dispatch",
    )(tokens_b, norm_gain[None], id_rows)

    arrived = lax.all_to_all(
        outgoing.reshape(EXPERTS, CAP, width), ("ep", "tp"), 0, 0, axis_index_groups=plane
    )
    everyone = lax.all_gather(
        arrived.reshape(slots, width), "tp", axis=0, axis_index_groups=same_core
    )

    mine = lax.all_to_all(latent, "tp", 0, 0, axis_index_groups=same_core)
    other = lax.ppermute(mine, "tp", swap)

    block = jnp.arange(rows, dtype=jnp.int32) // own
    side = jnp.where(block < chips, core, 1 - core)
    positions = (
        lax.axis_index("ep") * rows
        + ((block % chips) * 2 + side) * own
        + jnp.arange(rows, dtype=jnp.int32) % own
    )
    inverse = THETA ** (-jnp.arange(0, ROPE_DIM, 2, dtype=F32) / ROPE_DIM)
    angles = positions.astype(F32)[:, None] * inverse[None, :]
    cosine, sine = jnp.cos(angles), jnp.sin(angles)
    cosine = jnp.concatenate([cosine, cosine], axis=1)
    sine = jnp.concatenate([-sine, sine], axis=1)

    project = pl.pallas_call(
        project_body,
        out_shape=(
            jax.ShapeDtypeStruct((rows + rows // 2, LANES), BF16),
            jax.ShapeDtypeStruct((2 * rows + rows // 2, LANES), BF16),
        ),
        scratch_shapes=[
            pltpu.VMEM((rows, q_latent.shape[1]), BF16),
            pltpu.VMEM((rows, kv_latent.shape[1]), BF16),
        ],
        compiler_params=params(),
        name="project",
    )
    q_own, kv_own = project(
        mine, other, w_query, w_key, w_value, query_gain[None], key_gain[None], cosine, sine
    )

    kv_all = [kv_own] + [lax.ppermute(kv_own, "ep", shift(d, 0)) for d in (1, 3, 2)]
    q_all = [q_own] + [lax.ppermute(q_own, "ep", shift(0, d)) for d in (1, 3, 2)]
    partial = pl.pallas_call(
        attend_body,
        out_shape=[jax.ShapeDtypeStruct((rows + 16, LANES), BF16)] * SIDE,
        scratch_shapes=[pltpu.VMEM((SIDE * rows, 2 * LANES), BF16)] * 3
        + [pltpu.VMEM((SIDE * rows, 2 * LANES), F32)],
        compiler_params=params(),
        name="attend",
    )(*q_all, *kv_all)
    parts = [partial[0]] + [
        lax.ppermute(p, "ep", shift(0, -d)) for p, d in zip(partial[1:], (1, 3, 2))
    ]

    picked = []
    for w in (w_down, w_gate, w_up):
        picked.append(lax.dynamic_index_in_dim(w, 1 - core, 0, False))
    down_twin, *twin = [lax.ppermute(w, "tp", swap) for w in picked]
    mix_twin = lax.ppermute(w_mix, "tp", swap)

    span = slots + own
    step = chips // 2
    hidden = w_gate.shape[2]
    terms = pl.pallas_call(
        expert_body,
        out_shape=jax.ShapeDtypeStruct((chips, span, width), BF16),
        grid_spec=pltpu.PrefetchScalarGridSpec(
            num_scalar_prefetch=1,
            grid=(chips // step,),
            in_specs=[
                pl.BlockSpec((step, slots, width), lambda j, c: (j, 0, 0)),
                pl.BlockSpec((1, width, hidden), lambda j, c: (c[0], 0, 0)),
                pl.BlockSpec((1, width, hidden), lambda j, c: (c[0], 0, 0)),
                pl.BlockSpec((1, hidden, width), lambda j, c: (c[0], 0, 0)),
                pl.BlockSpec((width, hidden), lambda j, c: (0, 0)),
                pl.BlockSpec((width, hidden), lambda j, c: (0, 0)),
                pl.BlockSpec((hidden, width), lambda j, c: (0, 0)),
            ],
            out_specs=pl.BlockSpec((step, slots, width), lambda j, c: (j, 0, 0)),
        ),
        compiler_params=params(),
        name="experts",
    )(core.reshape(1), everyone, w_gate, w_up, w_down, *twin, down_twin)

    own_head, twin_head = pl.pallas_call(
        join_body,
        out_shape=[jax.ShapeDtypeStruct((half, VALUE_DIM), BF16)] * 2,
        compiler_params=params(),
        name="join",
    )(*parts)
    twin_head = lax.ppermute(twin_head, "tp", swap)
    terms = pl.pallas_call(
        mix_body,
        out_shape=jax.ShapeDtypeStruct((chips, span, width), BF16),
        in_specs=[pl.BlockSpec(memory_space=pltpu.VMEM)] * 4
        + [pl.BlockSpec(memory_space=pl.ANY)],
        out_specs=pl.BlockSpec(memory_space=pl.ANY),
        scratch_shapes=[
            pltpu.VMEM((half, width), BF16),
            pltpu.SemaphoreType.DMA((chips,)),
        ],
        input_output_aliases={4: 0},
        compiler_params=params(),
        name="mix",
    )(own_head, twin_head, w_mix, mix_twin, terms)

    summed = lax.psum_scatter(
        terms.reshape(chips * span, width),
        "tp",
        scatter_dimension=0,
        tiled=True,
        axis_index_groups=same_core,
    )
    mix_out = summed[slots:]
    returned = lax.all_to_all(
        summed.reshape(span // CAP, CAP, width)[:EXPERTS], ("ep", "tp"), 0, 0, axis_index_groups=plane
    )
    expert_out = pl.pallas_call(
        collect_body,
        out_shape=jax.ShapeDtypeStruct((own, width), BF16),
        compiler_params=params(),
        name="collect",
    )(returned.reshape(slots, width), id_rows, route_weights.T)
    return (mix_out, expert_out)


def solution(mesh):
    in_specs = (
        P(("ep", "tp"), None),
        P(("ep", "tp"), None),
        P(("ep", "tp"), None),
        P(),
        P(),
        P(None, "tp"),
        P(None, "tp"),
        P(None, "tp"),
        P(),
        P(),
        P("tp", None),
        P(("ep", "tp"), None),
        P(),
        P(("ep", "tp"), None),
        P(("ep", "tp"), None),
        P("ep", None, "tp"),
        P("ep", None, "tp"),
        P("ep", "tp", None),
    )
    out_specs = (P(("ep", "tp"), None), P(("ep", "tp"), None))

    return jax.shard_map(
        on_device, mesh=mesh, in_specs=in_specs, out_specs=out_specs, check_vma=False
    )
```

```python
import jax
import jax.numpy as jnp
from jax import lax
from jax.experimental import pallas as pl
from jax.experimental.pallas import tpu as pltpu
from jax.sharding import PartitionSpec as P


NOPE_DIM = 128
ROPE_DIM = 64
VALUE_DIM = 128
HEAD_DIM = NOPE_DIM + ROPE_DIM
EXPERTS = 32
TOP_K = 2
CAP = 4
SIDE = 4
EPSILON = 1e-06
THETA = 10000.0
LANES = 128
LOG2E = 1.4426950408889634


BF16 = jnp.bfloat16
F32 = jnp.float32


def params(mib=56):
    return pltpu.CompilerParams(vmem_limit_bytes=mib * 1024 * 1024)


def rms(values, gains):
    return values * lax.rsqrt(jnp.mean(values * values, axis=-1, keepdims=True) + EPSILON) * gains


def latent_body(q_ref, kv_ref, rope_ref, qg_ref, kvg_ref, out_ref):
    rows = q_ref.shape[0]
    q = rms(q_ref[...].astype(F32), qg_ref[...][None, :]).astype(BF16)
    kv = rms(kv_ref[...].astype(F32), kvg_ref[...]).astype(BF16)
    rope = rope_ref[...]
    parts = [p[:, j : j + LANES] for p in (q, kv) for j in range(0, p.shape[1], LANES)]
    parts.append(jnp.concatenate([rope, jnp.zeros_like(rope)], axis=1))
    for n, part in enumerate(parts):
        for peer in range(out_ref.shape[0]):
            out_ref[peer, n * rows : (n + 1) * rows, :] = part


def square(row):
    return jnp.broadcast_to(row, (row.shape[1], row.shape[1]))


def slots_of(rows, as_rows):
    count = rows.shape[1]
    line = lax.broadcasted_iota(jnp.int32, (count, count), 0)
    lane = lax.broadcasted_iota(jnp.int32, (count, count), 1)
    ids = [square(rows[k : k + 1, :].astype(F32)) for k in range(TOP_K)]
    outs = []
    for k in range(TOP_K):
        if as_rows:
            same = sum(jnp.where((p.T == ids[k]) & (line < lane), 1.0, 0.0) for p in ids)
            picked = ids[k][:1, :] * CAP + jnp.sum(same, axis=0, keepdims=True)
        else:
            mine = ids[k].T
            same = sum(jnp.where((p == mine) & (lane < line), 1.0, 0.0) for p in ids)
            picked = mine[:, :1] * CAP + jnp.sum(same, axis=1, keepdims=True)
        outs.append(picked.astype(jnp.int32))
    return outs


def dispatch_body(tok_ref, gain_ref, rows_ref, out_ref):
    normed = rms(tok_ref[...].astype(F32), gain_ref[...]).astype(BF16)
    first, second = slots_of(rows_ref[...], True)
    experts, cap, width = out_ref.shape
    shape = (experts * cap, normed.shape[0])
    slot = lax.broadcasted_iota(jnp.int32, shape, 0)
    hot = jnp.where((slot == first) | (slot == second), 1.0, 0.0).astype(BF16)
    picked = jnp.dot(hot, normed, preferred_element_type=F32)
    out_ref[...] = picked.reshape(experts, cap, width).astype(BF16)


def collect_body(back_ref, rows_ref, weight_ref, out_ref):
    first, second = slots_of(rows_ref[...], False)
    count = out_ref.shape[0]
    slots = back_ref.shape[0] * back_ref.shape[1]
    slot = lax.broadcasted_iota(jnp.int32, (count, slots), 1)
    weights = [square(weight_ref[k : k + 1, :]).T[:, :1] for k in range(TOP_K)]
    mixed = jnp.where(slot == first, weights[0], 0.0) + jnp.where(slot == second, weights[1], 0.0)
    high = mixed.astype(BF16)
    rest = mixed - high.astype(F32)
    low = rest.astype(BF16)
    last = (rest - low.astype(F32)).astype(BF16)
    back = back_ref[...].astype(F32).reshape(slots, back_ref.shape[2]).astype(BF16)
    total = jnp.dot(high, back, preferred_element_type=F32)
    total += jnp.dot(low, back, preferred_element_type=F32)
    total += jnp.dot(last, back, preferred_element_type=F32)
    out_ref[...] = total.astype(BF16)


def turned(values, cosine, sine):
    half = values.shape[-1] // 2
    swapped = jnp.concatenate([values[:, half:], values[:, :half]], axis=1)
    return values * cosine + swapped * sine


def project_body(
    mine_ref, other_ref, wq_ref, wk_ref, wv_ref, qg_ref, kg_ref, cos_ref, sin_ref,
    q_ref, kv_ref, lat_q, lat_kv,
):
    groups, height, _ = mine_ref.shape
    q_parts = lat_q.shape[1] // LANES
    kv_parts = lat_kv.shape[1] // LANES
    own = height // (q_parts + kv_parts + 1)
    half = groups * own
    ropes = []
    for n, src in enumerate((mine_ref, other_ref)):
        for j in range(q_parts + kv_parts):
            piece = src[:, j * own : (j + 1) * own, :].reshape(half, LANES)
            dst, col = (lat_q, j) if j < q_parts else (lat_kv, j - q_parts)
            dst[n * half : (n + 1) * half, col * LANES : (col + 1) * LANES] = piece
        ropes.append(src[:, (q_parts + kv_parts) * own :, :].reshape(half, LANES)[:, :ROPE_DIM])
    rope = jnp.concatenate(ropes, axis=0).astype(F32)
    cosine, sine = cos_ref[...], sin_ref[...]
    queries = lax.dot_general(
        lat_q[...], wq_ref[...], (((1,), (1,)), ((), ())), preferred_element_type=F32
    )
    scale = HEAD_DIM**-0.5 * LOG2E
    queries = rms(queries, qg_ref[...] * scale)
    q_ref[: 2 * half, :] = queries[:, :NOPE_DIM].astype(BF16)
    q_rope = turned(queries[:, NOPE_DIM:], cosine, sine).astype(BF16)
    q_ref[2 * half :, :] = jnp.concatenate([q_rope[:half], q_rope[half:]], axis=1)
    latent = lat_kv[...]
    keys = jnp.dot(latent, wk_ref[...], preferred_element_type=F32)
    square = jnp.sum(keys * keys, axis=-1, keepdims=True) + jnp.sum(
        rope * rope, axis=-1, keepdims=True
    )
    factor = lax.rsqrt(square / HEAD_DIM + EPSILON)
    gains = kg_ref[...]
    kv_ref[: 2 * half, :] = (keys * factor * gains[:, :NOPE_DIM]).astype(BF16)
    kv_ref[2 * half : 4 * half, :] = jnp.dot(
        latent, wv_ref[...], preferred_element_type=F32
    ).astype(BF16)
    k_rope = turned(rope * factor * gains[:, NOPE_DIM:], cosine, sine).astype(BF16)
    kv_ref[4 * half :, :] = jnp.concatenate([k_rope[:half], k_rope[half:]], axis=1)


def attend_body(*refs):
    q_refs, kv_refs, out_refs = refs[:SIDE], refs[SIDE : 2 * SIDE], refs[2 * SIDE : 3 * SIDE]
    qs, ks, vs, acc_ref = refs[3 * SIDE :]
    rows = qs.shape[0] // SIDE
    half = rows // 2
    zero = jnp.zeros((half, ROPE_DIM), BF16)
    ones = jnp.ones((rows, LANES), BF16)
    for b in range(SIDE):
        at = b * rows
        for src, dst, off in ((q_refs[b], qs, rows), (kv_refs[b], ks, 2 * rows)):
            dst[at : at + rows, :NOPE_DIM] = src[:rows, :]
            packed = src[off : off + half, :]
            dst[at : at + half, NOPE_DIM:] = jnp.concatenate([packed[:, :ROPE_DIM], zero], axis=1)
            dst[at + half : at + rows, NOPE_DIM:] = jnp.concatenate(
                [packed[:, ROPE_DIM:], zero], axis=1
            )
        vs[at : at + rows, :VALUE_DIM] = kv_refs[b][rows : 2 * rows, :]
        vs[at : at + rows, VALUE_DIM:] = ones

    def block(i, carry):
        here = pl.ds(pl.multiple_of(i * rows, rows), rows)
        q = qs[here, :]
        acc = None
        for b in range(SIDE):
            there = slice(b * rows, (b + 1) * rows)
            scores = lax.dot_general(
                q, ks[there, :], (((1,), (1,)), ((), ())), preferred_element_type=F32
            )
            probs = jnp.exp2(scores).astype(BF16)
            term = jnp.dot(probs, vs[there, :], preferred_element_type=F32)
            acc = term if acc is None else acc + term
        acc_ref[here, :] = acc
        return carry

    lax.fori_loop(0, SIDE, block, 0)
    for b in range(SIDE):
        at = b * rows
        out_refs[b][:rows, :] = acc_ref[at : at + rows, :VALUE_DIM].astype(BF16)
        for j in range(rows // LANES):
            total = acc_ref[at + j * LANES : at + (j + 1) * LANES, VALUE_DIM:].T[0:1, :]
            high = total.astype(BF16)
            low = (total - high.astype(F32)).astype(BF16)
            out_refs[b][rows + j : rows + j + 1, :] = high
            out_refs[b][rows + 8 + j : rows + 8 + j + 1, :] = low


def join_body(*refs):
    parts, outs = refs[:SIDE], refs[SIDE:]
    half = outs[0].shape[0]
    rows = 2 * half
    total = sum(
        p[rows : rows + 8, :].astype(F32) + p[rows + 8 : rows + 16, :].astype(F32) for p in parts
    )
    inverse = 1.0 / total
    for j in range(rows // LANES):
        there = slice(j * LANES, (j + 1) * LANES)
        scale = jnp.broadcast_to(inverse[j : j + 1, :], (LANES, LANES)).T
        head = sum(p[there, :].astype(F32) for p in parts)
        at = j * LANES % half
        outs[j * LANES // half][at : at + LANES, :] = (head * scale).astype(BF16)


def mix_body(own_ref, twin_ref, w_own_ref, w_twin_ref, _, out_ref, term_ref, sems):
    owners, span, _ = out_ref.shape
    each = own_ref.shape[0] // owners
    step = owners // 2
    copies = []
    for c in range(2):
        there = slice(c * step * each, (c + 1) * step * each)
        term = jnp.dot(own_ref[there, :], w_own_ref[...], preferred_element_type=F32)
        term += jnp.dot(twin_ref[there, :], w_twin_ref[...], preferred_element_type=F32)
        term_ref[there, :] = term.astype(BF16)
        for i in range(c * step, (c + 1) * step):
            copy = pltpu.make_async_copy(
                term_ref.at[pl.ds(i * each, each), :],
                out_ref.at[i, pl.ds(span - each, each), :],
                sems.at[i],
            )
            copy.start()
            copies.append(copy)
    for copy in copies:
        copy.wait()


def expert_body(core_ref, x_ref, *refs):
    del core_ref
    sets, out_ref = (refs[:3], refs[3:6]), refs[6]
    groups, rows, width = x_ref.shape
    x = x_ref[...].reshape(groups * rows, width)
    out = None
    for gate_ref, up_ref, down_ref in sets:
        gate = jnp.dot(x, gate_ref[...].reshape(width, -1), preferred_element_type=F32)
        up = jnp.dot(x, up_ref[...].reshape(width, -1), preferred_element_type=F32)
        hidden = (gate / (1.0 + jnp.exp(-gate)) * up).astype(BF16)
        term = jnp.dot(hidden, down_ref[...].reshape(-1, width), preferred_element_type=F32)
        out = term if out is None else out + term
    out_ref[...] = out.astype(BF16).reshape(groups, rows, width)


def shift(keys, queries, tp_count):
    pairs = []
    for e in range(SIDE * SIDE):
        for t in range(tp_count):
            step_x, step_y = (keys, queries) if t % 2 == 0 else (queries, keys)
            there = (e // SIDE + step_y) % SIDE * SIDE + (e % SIDE + step_x) % SIDE
            pairs.append((e * tp_count + t, there * tp_count + t))
    return pairs


def on_device(
    q_latent,
    kv_latent,
    rope_key,
    q_latent_gain,
    kv_latent_gain,
    w_query,
    w_key,
    w_value,
    query_gain,
    key_gain,
    w_mix,
    tokens_b,
    norm_gain,
    expert_ids,
    route_weights,
    w_gate,
    w_up,
    w_down,
):
    tp_count = lax.axis_size("tp")
    ep_count = lax.axis_size("ep")
    chips = tp_count // 2
    own = q_latent.shape[0]
    rows = own * tp_count
    half = rows // 2
    width = tokens_b.shape[1]
    slots = EXPERTS * CAP
    tp_at = lax.axis_index("tp")
    core = tp_at % 2
    same_core = [[z * 2 + c for z in range(chips)] for c in range(2)]
    plane = [
        [e * tp_count + z * 2 + c for e in range(ep_count) for c in range(2)] for z in range(chips)
    ]
    swap = [(i, i ^ 1) for i in range(tp_count)]

    def move(x, keys, queries):
        return lax.ppermute(x, ("ep", "tp"), shift(keys, queries, tp_count))


    height = own * ((q_latent.shape[1] + kv_latent.shape[1]) // LANES + 1)
    latent = pl.pallas_call(
        latent_body,
        out_shape=jax.ShapeDtypeStruct((chips, height, LANES), BF16),
        compiler_params=params(),
        name="latents",
    )(q_latent, kv_latent, rope_key, q_latent_gain, kv_latent_gain[None])

    latent, tokens_b = lax.optimization_barrier((latent, tokens_b))
    id_rows = expert_ids.T
    dispatch = pl.pallas_call(
        dispatch_body,
        out_shape=jax.ShapeDtypeStruct((EXPERTS, CAP, width), BF16),
        compiler_params=params(),
        name="dispatch",
    )
    outgoing = dispatch(tokens_b, norm_gain[None], id_rows)

    arrived = lax.all_to_all(
        outgoing, ("ep", "tp"), 0, 0, axis_index_groups=plane
    )
    everyone = lax.all_gather(
        arrived.reshape(slots, width), "tp", axis=0, axis_index_groups=same_core
    )

    mine = lax.all_to_all(latent, "tp", 0, 0, axis_index_groups=same_core)
    other = lax.ppermute(mine, "tp", swap)

    block = jnp.arange(rows, dtype=jnp.int32) // own
    side = jnp.where(block < chips, core, 1 - core)
    positions = (
        lax.axis_index("ep") * rows
        + ((block % chips) * 2 + side) * own
        + jnp.arange(rows, dtype=jnp.int32) % own
    )
    inverse = THETA ** (-jnp.arange(0, ROPE_DIM, 2, dtype=F32) / ROPE_DIM)
    angles = positions.astype(F32)[:, None] * inverse[None, :]
    cosine, sine = jnp.cos(angles), jnp.sin(angles)
    cosine = jnp.concatenate([cosine, cosine], axis=1)
    sine = jnp.concatenate([-sine, sine], axis=1)

    project = pl.pallas_call(
        project_body,
        out_shape=(
            jax.ShapeDtypeStruct((rows + rows // 2, LANES), BF16),
            jax.ShapeDtypeStruct((2 * rows + rows // 2, LANES), BF16),
        ),
        scratch_shapes=[
            pltpu.VMEM((rows, q_latent.shape[1]), BF16),
            pltpu.VMEM((rows, kv_latent.shape[1]), BF16),
        ],
        compiler_params=params(),
        name="project",
    )
    q_own, kv_own = project(
        mine, other, w_query.T, w_key, w_value, query_gain[None], key_gain[None], cosine, sine
    )

    kv_all = [kv_own] + [move(kv_own, d, 0) for d in (1, 3, 2)]
    q_all = [q_own] + [move(q_own, 0, d) for d in (1, 3, 2)]
    partial = pl.pallas_call(
        attend_body,
        out_shape=[jax.ShapeDtypeStruct((rows + 16, LANES), BF16)] * SIDE,
        scratch_shapes=[pltpu.VMEM((SIDE * rows, 2 * LANES), BF16)] * 3
        + [pltpu.VMEM((SIDE * rows, 2 * LANES), F32)],
        compiler_params=params(),
        name="attend",
    )(*q_all, *kv_all)
    parts = [partial[0]] + [
        move(p, 0, -d) for p, d in zip(partial[1:], (1, 3, 2))
    ]

    picked = []
    for w in (w_down, w_gate, w_up):
        picked.append(lax.dynamic_index_in_dim(w, 1 - core, 0, False))
    down_twin, *twin = [lax.ppermute(w, "tp", swap) for w in picked]
    mix_twin = lax.ppermute(w_mix, "tp", swap)

    span = slots + own
    step = chips // 2
    hidden = w_gate.shape[2]
    terms = pl.pallas_call(
        expert_body,
        out_shape=jax.ShapeDtypeStruct((chips, span, width), BF16),
        grid_spec=pltpu.PrefetchScalarGridSpec(
            num_scalar_prefetch=1,
            grid=(chips // step,),
            in_specs=[
                pl.BlockSpec((step, slots, width), lambda j, c: (j, 0, 0)),
                pl.BlockSpec((1, width, hidden), lambda j, c: (c[0], 0, 0)),
                pl.BlockSpec((1, width, hidden), lambda j, c: (c[0], 0, 0)),
                pl.BlockSpec((1, hidden, width), lambda j, c: (c[0], 0, 0)),
                pl.BlockSpec((width, hidden), lambda j, c: (0, 0)),
                pl.BlockSpec((width, hidden), lambda j, c: (0, 0)),
                pl.BlockSpec((hidden, width), lambda j, c: (0, 0)),
            ],
            out_specs=pl.BlockSpec((step, slots, width), lambda j, c: (j, 0, 0)),
        ),
        compiler_params=params(),
        name="experts",
    )(core.reshape(1), everyone, w_gate, w_up, w_down, *twin, down_twin)

    own_head, twin_head = pl.pallas_call(
        join_body,
        out_shape=[jax.ShapeDtypeStruct((half, VALUE_DIM), BF16)] * 2,
        compiler_params=params(),
        name="join",
    )(*parts)
    twin_head = lax.ppermute(twin_head, "tp", swap)
    terms = pl.pallas_call(
        mix_body,
        out_shape=jax.ShapeDtypeStruct((chips, span, width), BF16),
        in_specs=[pl.BlockSpec(memory_space=pltpu.VMEM)] * 4
        + [pl.BlockSpec(memory_space=pl.ANY)],
        out_specs=pl.BlockSpec(memory_space=pl.ANY),
        scratch_shapes=[
            pltpu.VMEM((half, width), BF16),
            pltpu.SemaphoreType.DMA((chips,)),
        ],
        input_output_aliases={4: 0},
        compiler_params=params(),
        name="mix",
    )(own_head, twin_head, w_mix, mix_twin, terms)

    summed = lax.psum_scatter(
        terms.reshape(chips * span, width),
        "tp",
        scatter_dimension=0,
        tiled=True,
        axis_index_groups=same_core,
    )
    mix_out = summed[slots:]
    returned = lax.all_to_all(
        summed.reshape(span // CAP, CAP, width)[:EXPERTS], ("ep", "tp"), 0, 0, axis_index_groups=plane
    )
    expert_out = pl.pallas_call(
        collect_body,
        out_shape=jax.ShapeDtypeStruct((own, width), BF16),
        compiler_params=params(),
        name="collect",
    )(returned, id_rows, route_weights.T)
    return (mix_out, expert_out)


def solution(mesh):
    in_specs = (
        P(("ep", "tp"), None),
        P(("ep", "tp"), None),
        P(("ep", "tp"), None),
        P(),
        P(),
        P(None, "tp"),
        P(None, "tp"),
        P(None, "tp"),
        P(),
        P(),
        P("tp", None),
        P(("ep", "tp"), None),
        P(),
        P(("ep", "tp"), None),
        P(("ep", "tp"), None),
        P("ep", None, "tp"),
        P("ep", None, "tp"),
        P("ep", "tp", None),
    )
    out_specs = (P(("ep", "tp"), None), P(("ep", "tp"), None))

    return jax.shard_map(
        on_device, mesh=mesh, in_specs=in_specs, out_specs=out_specs, check_vma=False
    )
```

```python
import jax
import jax.numpy as jnp
from jax import lax
from jax.experimental import pallas as pl
from jax.experimental.pallas import tpu as pltpu
from jax.sharding import PartitionSpec as P


NOPE_DIM = 128
ROPE_DIM = 64
VALUE_DIM = 128
HEAD_DIM = NOPE_DIM + ROPE_DIM
EXPERTS = 32
TOP_K = 2
CAP = 4
SIDE = 4
EPSILON = 1e-06
THETA = 10000.0
LANES = 128
LOG2E = 1.4426950408889634


BF16 = jnp.bfloat16
F32 = jnp.float32


def params(mib=56):
    return pltpu.CompilerParams(vmem_limit_bytes=mib * 1024 * 1024)


def rms(values, gains):
    return values * lax.rsqrt(jnp.mean(values * values, axis=-1, keepdims=True) + EPSILON) * gains


def latent_body(q_ref, kv_ref, rope_ref, qg_ref, kvg_ref, out_ref):
    rows = q_ref.shape[0]
    q = rms(q_ref[...].astype(F32), qg_ref[...][None, :]).astype(BF16)
    kv = rms(kv_ref[...].astype(F32), kvg_ref[...]).astype(BF16)
    rope = rope_ref[...]
    parts = [p[:, j : j + LANES] for p in (q, kv) for j in range(0, p.shape[1], LANES)]
    parts.append(jnp.concatenate([rope, jnp.zeros_like(rope)], axis=1))
    for n, part in enumerate(parts):
        for peer in range(out_ref.shape[0]):
            out_ref[peer, n * rows : (n + 1) * rows, :] = part


def square(row):
    return jnp.broadcast_to(row, (row.shape[1], row.shape[1]))


def slots_of(rows, as_rows):
    count = rows.shape[1]
    line = lax.broadcasted_iota(jnp.int32, (count, count), 0)
    lane = lax.broadcasted_iota(jnp.int32, (count, count), 1)
    ids = [square(rows[k : k + 1, :].astype(F32)) for k in range(TOP_K)]
    outs = []
    for k in range(TOP_K):
        if as_rows:
            same = sum(jnp.where((p.T == ids[k]) & (line < lane), 1.0, 0.0) for p in ids)
            picked = ids[k][:1, :] * CAP + jnp.sum(same, axis=0, keepdims=True)
        else:
            mine = ids[k].T
            same = sum(jnp.where((p == mine) & (lane < line), 1.0, 0.0) for p in ids)
            picked = mine[:, :1] * CAP + jnp.sum(same, axis=1, keepdims=True)
        outs.append(picked.astype(jnp.int32))
    return outs


def dispatch_body(tok_ref, gain_ref, rows_ref, out_ref):
    normed = rms(tok_ref[...].astype(F32), gain_ref[...]).astype(BF16)
    first, second = slots_of(rows_ref[...], True)
    experts, cap, width = out_ref.shape
    shape = (experts * cap, normed.shape[0])
    slot = lax.broadcasted_iota(jnp.int32, shape, 0)
    hot = jnp.where((slot == first) | (slot == second), 1.0, 0.0).astype(BF16)
    picked = jnp.dot(hot, normed, preferred_element_type=F32)
    out_ref[...] = picked.reshape(experts, cap, width).astype(BF16)


def collect_body(back_ref, rows_ref, weight_ref, out_ref):
    first, second = slots_of(rows_ref[...], False)
    count = out_ref.shape[0]
    slots = back_ref.shape[0] * back_ref.shape[1]
    slot = lax.broadcasted_iota(jnp.int32, (count, slots), 1)
    weights = [square(weight_ref[k : k + 1, :]).T[:, :1] for k in range(TOP_K)]
    mixed = jnp.where(slot == first, weights[0], 0.0) + jnp.where(slot == second, weights[1], 0.0)
    high = mixed.astype(BF16)
    rest = mixed - high.astype(F32)
    low = rest.astype(BF16)
    last = (rest - low.astype(F32)).astype(BF16)
    back = back_ref[...].astype(F32).reshape(slots, back_ref.shape[2]).astype(BF16)
    total = jnp.dot(high, back, preferred_element_type=F32)
    total += jnp.dot(low, back, preferred_element_type=F32)
    total += jnp.dot(last, back, preferred_element_type=F32)
    out_ref[...] = total.astype(BF16)


def turned(values, cosine, sine):
    half = values.shape[-1] // 2
    swapped = jnp.concatenate([values[:, half:], values[:, :half]], axis=1)
    return values * cosine + swapped * sine


def project_body(
    mine_ref, other_ref, wq_ref, wk_ref, wv_ref, qg_ref, kg_ref, cos_ref, sin_ref,
    q_ref, kv_ref, lat_q, lat_kv,
):
    groups, height, _ = mine_ref.shape
    q_parts = lat_q.shape[1] // LANES
    kv_parts = lat_kv.shape[1] // LANES
    own = height // (q_parts + kv_parts + 1)
    half = groups * own
    ropes = []
    for n, src in enumerate((mine_ref, other_ref)):
        for j in range(q_parts + kv_parts):
            piece = src[:, j * own : (j + 1) * own, :].reshape(half, LANES)
            dst, col = (lat_q, j) if j < q_parts else (lat_kv, j - q_parts)
            dst[n * half : (n + 1) * half, col * LANES : (col + 1) * LANES] = piece
        ropes.append(src[:, (q_parts + kv_parts) * own :, :].reshape(half, LANES)[:, :ROPE_DIM])
    rope = jnp.concatenate(ropes, axis=0).astype(F32)
    cosine, sine = cos_ref[...], sin_ref[...]
    queries = lax.dot_general(
        lat_q[...], wq_ref[...], (((1,), (1,)), ((), ())), preferred_element_type=F32
    )
    scale = HEAD_DIM**-0.5 * LOG2E
    queries = rms(queries, qg_ref[...] * scale)
    q_ref[: 2 * half, :] = queries[:, :NOPE_DIM].astype(BF16)
    q_rope = turned(queries[:, NOPE_DIM:], cosine, sine).astype(BF16)
    q_ref[2 * half :, :] = jnp.concatenate([q_rope[:half], q_rope[half:]], axis=1)
    latent = lat_kv[...]
    keys = jnp.dot(latent, wk_ref[...], preferred_element_type=F32)
    square = jnp.sum(keys * keys, axis=-1, keepdims=True) + jnp.sum(
        rope * rope, axis=-1, keepdims=True
    )
    factor = lax.rsqrt(square / HEAD_DIM + EPSILON)
    gains = kg_ref[...]
    kv_ref[: 2 * half, :] = (keys * factor * gains[:, :NOPE_DIM]).astype(BF16)
    kv_ref[2 * half : 4 * half, :] = jnp.dot(
        latent, wv_ref[...], preferred_element_type=F32
    ).astype(BF16)
    k_rope = turned(rope * factor * gains[:, NOPE_DIM:], cosine, sine).astype(BF16)
    kv_ref[4 * half :, :] = jnp.concatenate([k_rope[:half], k_rope[half:]], axis=1)


def attend_body(*refs):
    q_refs, kv_refs, out_refs = refs[:SIDE], refs[SIDE : 2 * SIDE], refs[2 * SIDE : 3 * SIDE]
    qs, ks, vs, acc_ref = refs[3 * SIDE :]
    rows = qs.shape[0] // SIDE
    half = rows // 2
    zero = jnp.zeros((half, ROPE_DIM), BF16)
    ones = jnp.ones((rows, LANES), BF16)
    for b in range(SIDE):
        at = b * rows
        for src, dst, off in ((q_refs[b], qs, rows), (kv_refs[b], ks, 2 * rows)):
            dst[at : at + rows, :NOPE_DIM] = src[:rows, :]
            packed = src[off : off + half, :]
            dst[at : at + half, NOPE_DIM:] = jnp.concatenate([packed[:, :ROPE_DIM], zero], axis=1)
            dst[at + half : at + rows, NOPE_DIM:] = jnp.concatenate(
                [packed[:, ROPE_DIM:], zero], axis=1
            )
        vs[at : at + rows, :VALUE_DIM] = kv_refs[b][rows : 2 * rows, :]
        vs[at : at + rows, VALUE_DIM:] = ones

    def block(i, carry):
        here = pl.ds(pl.multiple_of(i * rows, rows), rows)
        q = qs[here, :]
        acc = None
        for b in range(SIDE):
            there = slice(b * rows, (b + 1) * rows)
            scores = lax.dot_general(
                q, ks[there, :], (((1,), (1,)), ((), ())), preferred_element_type=F32
            )
            probs = jnp.exp2(scores).astype(BF16)
            term = jnp.dot(probs, vs[there, :], preferred_element_type=F32)
            acc = term if acc is None else acc + term
        acc_ref[here, :] = acc
        return carry

    lax.fori_loop(0, SIDE, block, 0)
    for b in range(SIDE):
        at = b * rows
        out_refs[b][:rows, :] = acc_ref[at : at + rows, :VALUE_DIM].astype(BF16)
        for j in range(rows // LANES):
            total = acc_ref[at + j * LANES : at + (j + 1) * LANES, VALUE_DIM:].T[0:1, :]
            high = total.astype(BF16)
            low = (total - high.astype(F32)).astype(BF16)
            out_refs[b][rows + j : rows + j + 1, :] = high
            out_refs[b][rows + 8 + j : rows + 8 + j + 1, :] = low


def join_body(*refs):
    parts, outs = refs[:SIDE], refs[SIDE:]
    half = outs[0].shape[0]
    rows = 2 * half
    total = sum(
        p[rows : rows + 8, :].astype(F32) + p[rows + 8 : rows + 16, :].astype(F32) for p in parts
    )
    inverse = 1.0 / total
    for j in range(rows // LANES):
        there = slice(j * LANES, (j + 1) * LANES)
        scale = jnp.broadcast_to(inverse[j : j + 1, :], (LANES, LANES)).T
        head = sum(p[there, :].astype(F32) for p in parts)
        at = j * LANES % half
        outs[j * LANES // half][at : at + LANES, :] = (head * scale).astype(BF16)


def mix_body(own_ref, twin_ref, w_own_ref, w_twin_ref, out_ref):
    term = jnp.dot(own_ref[...], w_own_ref[...], preferred_element_type=F32)
    term += jnp.dot(twin_ref[...], w_twin_ref[...], preferred_element_type=F32)
    out_ref[...] = term.astype(BF16)


def expert_body(core_ref, x_ref, *refs):
    del core_ref
    sets, out_ref = (refs[:3], refs[3:6]), refs[6]
    groups, rows, width = x_ref.shape
    x = x_ref[...].reshape(groups * rows, width)
    out = None
    for gate_ref, up_ref, down_ref in sets:
        gate = jnp.dot(x, gate_ref[...].reshape(width, -1), preferred_element_type=F32)
        up = jnp.dot(x, up_ref[...].reshape(width, -1), preferred_element_type=F32)
        hidden = (gate / (1.0 + jnp.exp(-gate)) * up).astype(BF16)
        term = jnp.dot(hidden, down_ref[...].reshape(-1, width), preferred_element_type=F32)
        out = term if out is None else out + term
    out_ref[...] = out.astype(BF16).reshape(groups, rows, width)


def shift(keys, queries, tp_count):
    pairs = []
    for e in range(SIDE * SIDE):
        for t in range(tp_count):
            step_x, step_y = (keys, queries) if t % 2 == 0 else (queries, keys)
            there = (e // SIDE + step_y) % SIDE * SIDE + (e % SIDE + step_x) % SIDE
            pairs.append((e * tp_count + t, there * tp_count + t))
    return pairs


def on_device(
    q_latent,
    kv_latent,
    rope_key,
    q_latent_gain,
    kv_latent_gain,
    w_query,
    w_key,
    w_value,
    query_gain,
    key_gain,
    w_mix,
    tokens_b,
    norm_gain,
    expert_ids,
    route_weights,
    w_gate,
    w_up,
    w_down,
):
    tp_count = lax.axis_size("tp")
    ep_count = lax.axis_size("ep")
    chips = tp_count // 2
    own = q_latent.shape[0]
    rows = own * tp_count
    half = rows // 2
    width = tokens_b.shape[1]
    slots = EXPERTS * CAP
    tp_at = lax.axis_index("tp")
    core = tp_at % 2
    same_core = [[z * 2 + c for z in range(chips)] for c in range(2)]
    plane = [
        [e * tp_count + z * 2 + c for e in range(ep_count) for c in range(2)] for z in range(chips)
    ]
    swap = [(i, i ^ 1) for i in range(tp_count)]

    def move(x, keys, queries):
        return lax.ppermute(x, ("ep", "tp"), shift(keys, queries, tp_count))


    height = own * ((q_latent.shape[1] + kv_latent.shape[1]) // LANES + 1)
    latents = pl.pallas_call(
        latent_body,
        out_shape=jax.ShapeDtypeStruct((chips, height, LANES), BF16),
        compiler_params=params(),
        name="latents",
    )
    latent = latents(q_latent, kv_latent, rope_key, q_latent_gain, kv_latent_gain[None])

    id_rows = expert_ids.T
    dispatch = pl.pallas_call(
        dispatch_body,
        out_shape=jax.ShapeDtypeStruct((EXPERTS, CAP, width), BF16),
        compiler_params=params(),
        name="dispatch",
    )
    outgoing = dispatch(tokens_b, norm_gain[None], id_rows)

    arrived = lax.all_to_all(
        outgoing, ("ep", "tp"), 0, 0, axis_index_groups=plane
    )
    everyone = lax.all_gather(
        arrived.reshape(slots, width), "tp", axis=0, axis_index_groups=same_core
    )

    mine = lax.all_to_all(latent, "tp", 0, 0, axis_index_groups=same_core)
    other = lax.ppermute(mine, "tp", swap)

    block = jnp.arange(rows, dtype=jnp.int32) // own
    side = jnp.where(block < chips, core, 1 - core)
    positions = (
        lax.axis_index("ep") * rows
        + ((block % chips) * 2 + side) * own
        + jnp.arange(rows, dtype=jnp.int32) % own
    )
    inverse = THETA ** (-jnp.arange(0, ROPE_DIM, 2, dtype=F32) / ROPE_DIM)
    angles = positions.astype(F32)[:, None] * inverse[None, :]
    cosine, sine = jnp.cos(angles), jnp.sin(angles)
    cosine = jnp.concatenate([cosine, cosine], axis=1)
    sine = jnp.concatenate([-sine, sine], axis=1)

    project = pl.pallas_call(
        project_body,
        out_shape=(
            jax.ShapeDtypeStruct((rows + rows // 2, LANES), BF16),
            jax.ShapeDtypeStruct((2 * rows + rows // 2, LANES), BF16),
        ),
        scratch_shapes=[
            pltpu.VMEM((rows, q_latent.shape[1]), BF16),
            pltpu.VMEM((rows, kv_latent.shape[1]), BF16),
        ],
        compiler_params=params(),
        name="project",
    )
    q_own, kv_own = project(
        mine, other, w_query.T, w_key, w_value, query_gain[None], key_gain[None], cosine, sine
    )

    kv_all = [kv_own] + [move(kv_own, d, 0) for d in (1, 3, 2)]
    q_all = [q_own] + [move(q_own, 0, d) for d in (1, 3, 2)]
    partial = pl.pallas_call(
        attend_body,
        out_shape=[jax.ShapeDtypeStruct((rows + 16, LANES), BF16)] * SIDE,
        scratch_shapes=[pltpu.VMEM((SIDE * rows, 2 * LANES), BF16)] * 3
        + [pltpu.VMEM((SIDE * rows, 2 * LANES), F32)],
        compiler_params=params(),
        name="attend",
    )(*q_all, *kv_all)
    parts = [partial[0]] + [
        move(p, 0, -d) for p, d in zip(partial[1:], (1, 3, 2))
    ]

    picked = []
    for w in (w_down, w_gate, w_up):
        picked.append(lax.dynamic_index_in_dim(w, 1 - core, 0, False))
    down_twin, *twin = [lax.ppermute(w, "tp", swap) for w in picked]
    mix_twin = lax.ppermute(w_mix, "tp", swap)

    step = chips // 2
    hidden = w_gate.shape[2]
    terms = pl.pallas_call(
        expert_body,
        out_shape=jax.ShapeDtypeStruct((chips, slots, width), BF16),
        grid_spec=pltpu.PrefetchScalarGridSpec(
            num_scalar_prefetch=1,
            grid=(chips // step,),
            in_specs=[
                pl.BlockSpec((step, slots, width), lambda j, c: (j, 0, 0)),
                pl.BlockSpec((1, width, hidden), lambda j, c: (c[0], 0, 0)),
                pl.BlockSpec((1, width, hidden), lambda j, c: (c[0], 0, 0)),
                pl.BlockSpec((1, hidden, width), lambda j, c: (c[0], 0, 0)),
                pl.BlockSpec((width, hidden), lambda j, c: (0, 0)),
                pl.BlockSpec((width, hidden), lambda j, c: (0, 0)),
                pl.BlockSpec((hidden, width), lambda j, c: (0, 0)),
            ],
            out_specs=pl.BlockSpec((step, slots, width), lambda j, c: (j, 0, 0)),
        ),
        compiler_params=params(),
        name="experts",
    )(core.reshape(1), everyone, w_gate, w_up, w_down, *twin, down_twin)

    own_head, twin_head = pl.pallas_call(
        join_body,
        out_shape=[jax.ShapeDtypeStruct((half, VALUE_DIM), BF16)] * 2,
        compiler_params=params(),
        name="join",
    )(*parts)
    twin_head = lax.ppermute(twin_head, "tp", swap)
    mixed = pl.pallas_call(
        mix_body,
        out_shape=jax.ShapeDtypeStruct((half, width), BF16),
        grid=(2,),
        in_specs=[pl.BlockSpec((half // 2, VALUE_DIM), lambda i: (i, 0))] * 2
        + [pl.BlockSpec((VALUE_DIM, width), lambda i: (0, 0))] * 2,
        out_specs=pl.BlockSpec((half // 2, width), lambda i: (i, 0)),
        compiler_params=params(),
        name="mix",
    )(own_head, twin_head, w_mix, mix_twin)

    def summed(x):
        return lax.psum_scatter(
            x, "tp", scatter_dimension=0, tiled=True, axis_index_groups=same_core
        )

    done = summed(terms.reshape(chips * slots, width))
    mix_out = summed(mixed)
    returned = lax.all_to_all(
        done.reshape(EXPERTS, CAP, width), ("ep", "tp"), 0, 0, axis_index_groups=plane
    )
    expert_out = pl.pallas_call(
        collect_body,
        out_shape=jax.ShapeDtypeStruct((own, width), BF16),
        compiler_params=params(),
        name="collect",
    )(returned, id_rows, route_weights.T)
    return (mix_out, expert_out)


def solution(mesh):
    in_specs = (
        P(("ep", "tp"), None),
        P(("ep", "tp"), None),
        P(("ep", "tp"), None),
        P(),
        P(),
        P(None, "tp"),
        P(None, "tp"),
        P(None, "tp"),
        P(),
        P(),
        P("tp", None),
        P(("ep", "tp"), None),
        P(),
        P(("ep", "tp"), None),
        P(("ep", "tp"), None),
        P("ep", None, "tp"),
        P("ep", None, "tp"),
        P("ep", "tp", None),
    )
    out_specs = (P(("ep", "tp"), None), P(("ep", "tp"), None))

    return jax.shard_map(
        on_device, mesh=mesh, in_specs=in_specs, out_specs=out_specs, check_vma=False
    )
```

```python
import jax
import jax.numpy as jnp
from jax import lax
from jax.experimental import pallas as pl
from jax.experimental.pallas import tpu as pltpu
from jax.sharding import PartitionSpec as P


NOPE_DIM = 128
ROPE_DIM = 64
VALUE_DIM = 128
HEAD_DIM = NOPE_DIM + ROPE_DIM
EXPERTS = 32
TOP_K = 2
CAP = 4
SIDE = 4
EPSILON = 1e-06
THETA = 10000.0
LANES = 128
LOG2E = 1.4426950408889634


BF16 = jnp.bfloat16
F32 = jnp.float32


def params(mib=56):
    return pltpu.CompilerParams(vmem_limit_bytes=mib * 1024 * 1024)


def rms(values, gains):
    return values * lax.rsqrt(jnp.mean(values * values, axis=-1, keepdims=True) + EPSILON) * gains


def latent_body(q_ref, kv_ref, rope_ref, qg_ref, kvg_ref, out_ref, turn_ref):
    rows = q_ref.shape[0]
    q = rms(q_ref[...].astype(F32), qg_ref[...][None, :]).astype(BF16)
    kv = rms(kv_ref[...].astype(F32), kvg_ref[...]).astype(BF16)
    parts = [p[:, j : j + LANES] for p in (q, kv) for j in range(0, p.shape[1], LANES)]
    for n, part in enumerate(parts):
        out_ref[n * rows : (n + 1) * rows, :] = part
    rope = rope_ref[...].astype(F32)
    packed = jnp.concatenate([rope[: rows // 2, :], rope[rows // 2 :, :]], axis=1)
    turn_ref[...] = packed.astype(BF16)


def square(row):
    return jnp.broadcast_to(row, (row.shape[1], row.shape[1]))


def slots_of(rows, as_rows):
    count = rows.shape[1]
    line = lax.broadcasted_iota(jnp.int32, (count, count), 0)
    lane = lax.broadcasted_iota(jnp.int32, (count, count), 1)
    ids = [square(rows[k : k + 1, :].astype(F32)) for k in range(TOP_K)]
    outs = []
    for k in range(TOP_K):
        if as_rows:
            same = sum(jnp.where((p.T == ids[k]) & (line < lane), 1.0, 0.0) for p in ids)
            picked = ids[k][:1, :] * CAP + jnp.sum(same, axis=0, keepdims=True)
        else:
            mine = ids[k].T
            same = sum(jnp.where((p == mine) & (lane < line), 1.0, 0.0) for p in ids)
            picked = mine[:, :1] * CAP + jnp.sum(same, axis=1, keepdims=True)
        outs.append(picked.astype(jnp.int32))
    return outs


def dispatch_body(tok_ref, gain_ref, rows_ref, out_ref):
    normed = rms(tok_ref[...].astype(F32), gain_ref[...]).astype(BF16)
    first, second = slots_of(rows_ref[...], True)
    experts, cap, width = out_ref.shape
    shape = (experts * cap, normed.shape[0])
    slot = lax.broadcasted_iota(jnp.int32, shape, 0)
    hot = jnp.where((slot == first) | (slot == second), 1.0, 0.0).astype(BF16)
    picked = jnp.dot(hot, normed, preferred_element_type=F32)
    out_ref[...] = picked.reshape(experts, cap, width).astype(BF16)


def collect_body(back_ref, rows_ref, weight_ref, out_ref):
    first, second = slots_of(rows_ref[...], False)
    count = out_ref.shape[0]
    slots = back_ref.shape[0] * back_ref.shape[1]
    slot = lax.broadcasted_iota(jnp.int32, (count, slots), 1)
    weights = [square(weight_ref[k : k + 1, :]).T[:, :1] for k in range(TOP_K)]
    mixed = jnp.where(slot == first, weights[0], 0.0) + jnp.where(slot == second, weights[1], 0.0)
    high = mixed.astype(BF16)
    rest = mixed - high.astype(F32)
    low = rest.astype(BF16)
    last = (rest - low.astype(F32)).astype(BF16)
    back = back_ref[...].astype(F32).reshape(slots, back_ref.shape[2]).astype(BF16)
    total = jnp.dot(high, back, preferred_element_type=F32)
    total += jnp.dot(low, back, preferred_element_type=F32)
    total += jnp.dot(last, back, preferred_element_type=F32)
    out_ref[...] = total.astype(BF16)


def turned(values, cosine, sine):
    half = values.shape[-1] // 2
    swapped = jnp.concatenate([values[:, half:], values[:, :half]], axis=1)
    return values * cosine + swapped * sine


def project_body(
    lat_ref, turn_ref, wq_ref, wk_ref, wv_ref, qg_ref, kg_ref, cos_ref, sin_ref,
    q_ref, kv_ref, lat_q, lat_kv, turns,
):
    peers, height, _ = lat_ref.shape
    q_parts = lat_q.shape[1] // LANES
    kv_parts = lat_kv.shape[1] // LANES
    own = height // (q_parts + kv_parts)
    half = peers * own // 2
    for t in range(peers):
        at = (t % 2) * half + t // 2 * own
        for j in range(q_parts + kv_parts):
            piece = lat_ref[t, j * own : (j + 1) * own, :]
            dst, col = (lat_q, j) if j < q_parts else (lat_kv, j - q_parts)
            dst[at : at + own, col * LANES : (col + 1) * LANES] = piece
        packed = turn_ref[t, :, :].astype(F32)
        turns[at : at + own // 2, :] = packed[:, :ROPE_DIM]
        turns[at + own // 2 : at + own, :] = packed[:, ROPE_DIM:]
    rope = turns[...]
    cosine, sine = cos_ref[...], sin_ref[...]
    queries = lax.dot_general(
        lat_q[...], wq_ref[...], (((1,), (1,)), ((), ())), preferred_element_type=F32
    )
    scale = HEAD_DIM**-0.5 * LOG2E
    queries = rms(queries, qg_ref[...] * scale)
    q_ref[: 2 * half, :] = queries[:, :NOPE_DIM].astype(BF16)
    q_rope = turned(queries[:, NOPE_DIM:], cosine, sine).astype(BF16)
    q_ref[2 * half :, :] = jnp.concatenate([q_rope[:half], q_rope[half:]], axis=1)
    latent = lat_kv[...]
    keys = jnp.dot(latent, wk_ref[...], preferred_element_type=F32)
    square = jnp.sum(keys * keys, axis=-1, keepdims=True) + jnp.sum(
        rope * rope, axis=-1, keepdims=True
    )
    factor = lax.rsqrt(square / HEAD_DIM + EPSILON)
    gains = kg_ref[...]
    kv_ref[: 2 * half, :] = (keys * factor * gains[:, :NOPE_DIM]).astype(BF16)
    kv_ref[2 * half : 4 * half, :] = jnp.dot(
        latent, wv_ref[...], preferred_element_type=F32
    ).astype(BF16)
    k_rope = turned(rope * factor * gains[:, NOPE_DIM:], cosine, sine).astype(BF16)
    kv_ref[4 * half :, :] = jnp.concatenate([k_rope[:half], k_rope[half:]], axis=1)


def attend_body(*refs):
    q_refs, kv_refs, out_refs = refs[:SIDE], refs[SIDE : 2 * SIDE], refs[2 * SIDE : 3 * SIDE]
    qs, ks, vs, acc_ref = refs[3 * SIDE :]
    rows = qs.shape[0] // SIDE
    half = rows // 2
    zero = jnp.zeros((half, ROPE_DIM), BF16)
    ones = jnp.ones((rows, LANES), BF16)
    for b in range(SIDE):
        at = b * rows
        for src, dst, off in ((q_refs[b], qs, rows), (kv_refs[b], ks, 2 * rows)):
            dst[at : at + rows, :NOPE_DIM] = src[:rows, :]
            packed = src[off : off + half, :]
            dst[at : at + half, NOPE_DIM:] = jnp.concatenate([packed[:, :ROPE_DIM], zero], axis=1)
            dst[at + half : at + rows, NOPE_DIM:] = jnp.concatenate(
                [packed[:, ROPE_DIM:], zero], axis=1
            )
        vs[at : at + rows, :VALUE_DIM] = kv_refs[b][rows : 2 * rows, :]
        vs[at : at + rows, VALUE_DIM:] = ones

    def block(i, carry):
        here = pl.ds(pl.multiple_of(i * rows, rows), rows)
        q = qs[here, :]
        acc = None
        for b in range(SIDE):
            there = slice(b * rows, (b + 1) * rows)
            scores = lax.dot_general(
                q, ks[there, :], (((1,), (1,)), ((), ())), preferred_element_type=F32
            )
            probs = jnp.exp2(scores).astype(BF16)
            term = jnp.dot(probs, vs[there, :], preferred_element_type=F32)
            acc = term if acc is None else acc + term
        acc_ref[here, :] = acc
        return carry

    lax.fori_loop(0, SIDE, block, 0)
    for b in range(SIDE):
        at = b * rows
        out_refs[b][:rows, :] = acc_ref[at : at + rows, :VALUE_DIM].astype(BF16)
        for j in range(rows // LANES):
            total = acc_ref[at + j * LANES : at + (j + 1) * LANES, VALUE_DIM:].T[0:1, :]
            high = total.astype(BF16)
            low = (total - high.astype(F32)).astype(BF16)
            out_refs[b][rows + j : rows + j + 1, :] = high
            out_refs[b][rows + 8 + j : rows + 8 + j + 1, :] = low


def join_body(core_ref, *refs):
    parts, (own_ref, twin_ref, head_ref) = refs[:SIDE], refs[SIDE:]
    half = own_ref.shape[0]
    rows = 2 * half
    total = sum(
        p[rows : rows + 8, :].astype(F32) + p[rows + 8 : rows + 16, :].astype(F32) for p in parts
    )
    inverse = 1.0 / total
    for j in range(rows // LANES):
        there = slice(j * LANES, (j + 1) * LANES)
        scale = jnp.broadcast_to(inverse[j : j + 1, :], (LANES, LANES)).T
        head = sum(p[there, :].astype(F32) for p in parts)
        head_ref[there, :] = (head * scale).astype(BF16)
    core = core_ref[0]
    own_ref[...] = head_ref[pl.ds(pl.multiple_of(core * half, half), half), :]
    twin_ref[...] = head_ref[pl.ds(pl.multiple_of((1 - core) * half, half), half), :]


def mix_body(own_ref, twin_ref, w_own_ref, w_twin_ref, out_ref):
    term = jnp.dot(own_ref[...], w_own_ref[...], preferred_element_type=F32)
    term += jnp.dot(twin_ref[...], w_twin_ref[...], preferred_element_type=F32)
    out_ref[...] = term.astype(BF16)


def expert_body(core_ref, x_ref, *refs):
    del core_ref
    sets, out_ref = (refs[:3], refs[3:6]), refs[6]
    groups, rows, width = x_ref.shape
    x = x_ref[...].reshape(groups * rows, width)
    out = None
    for gate_ref, up_ref, down_ref in sets:
        gate = jnp.dot(x, gate_ref[...].reshape(width, -1), preferred_element_type=F32)
        up = jnp.dot(x, up_ref[...].reshape(width, -1), preferred_element_type=F32)
        hidden = (gate / (1.0 + jnp.exp(-gate)) * up).astype(BF16)
        term = jnp.dot(hidden, down_ref[...].reshape(-1, width), preferred_element_type=F32)
        out = term if out is None else out + term
    out_ref[...] = out.astype(BF16).reshape(groups, rows, width)


def shift(keys, queries, tp_count):
    pairs = []
    for e in range(SIDE * SIDE):
        for t in range(tp_count):
            step_x, step_y = (keys, queries) if t % 2 == 0 else (queries, keys)
            there = (e // SIDE + step_y) % SIDE * SIDE + (e % SIDE + step_x) % SIDE
            pairs.append((e * tp_count + t, there * tp_count + t))
    return pairs


def on_device(
    q_latent,
    kv_latent,
    rope_key,
    q_latent_gain,
    kv_latent_gain,
    w_query,
    w_key,
    w_value,
    query_gain,
    key_gain,
    w_mix,
    tokens_b,
    norm_gain,
    expert_ids,
    route_weights,
    w_gate,
    w_up,
    w_down,
):
    tp_count = lax.axis_size("tp")
    ep_count = lax.axis_size("ep")
    chips = tp_count // 2
    own = q_latent.shape[0]
    rows = own * tp_count
    half = rows // 2
    width = tokens_b.shape[1]
    slots = EXPERTS * CAP
    tp_at = lax.axis_index("tp")
    core = tp_at % 2
    same_core = [[z * 2 + c for z in range(chips)] for c in range(2)]
    plane = [
        [e * tp_count + z * 2 + c for e in range(ep_count) for c in range(2)] for z in range(chips)
    ]
    swap = [(i, i ^ 1) for i in range(tp_count)]

    def move(x, keys, queries):
        return lax.ppermute(x, ("ep", "tp"), shift(keys, queries, tp_count))


    height = own * ((q_latent.shape[1] + kv_latent.shape[1]) // LANES)
    latents = pl.pallas_call(
        latent_body,
        out_shape=[
            jax.ShapeDtypeStruct((height, LANES), BF16),
            jax.ShapeDtypeStruct((own // 2, LANES), BF16),
        ],
        compiler_params=params(),
        name="latents",
    )
    latent, turn = latents(q_latent, kv_latent, rope_key, q_latent_gain, kv_latent_gain[None])

    id_rows = expert_ids.T
    dispatch = pl.pallas_call(
        dispatch_body,
        out_shape=jax.ShapeDtypeStruct((EXPERTS, CAP, width), BF16),
        compiler_params=params(),
        name="dispatch",
    )
    outgoing = dispatch(tokens_b, norm_gain[None], id_rows)

    arrived = lax.all_to_all(
        outgoing, ("ep", "tp"), 0, 0, axis_index_groups=plane
    )
    latent = lax.all_gather(latent, "tp", axis=0)
    arrived, turn = lax.optimization_barrier((arrived.reshape(slots, width), turn))
    everyone = lax.all_gather(arrived, "tp", axis=0, axis_index_groups=same_core)
    turn = lax.all_gather(turn, "tp", axis=0)

    block = jnp.arange(rows, dtype=jnp.int32) // own
    positions = (
        lax.axis_index("ep") * rows
        + ((block % chips) * 2 + block // chips) * own
        + jnp.arange(rows, dtype=jnp.int32) % own
    )
    inverse = THETA ** (-jnp.arange(0, ROPE_DIM, 2, dtype=F32) / ROPE_DIM)
    angles = positions.astype(F32)[:, None] * inverse[None, :]
    cosine, sine = jnp.cos(angles), jnp.sin(angles)
    cosine = jnp.concatenate([cosine, cosine], axis=1)
    sine = jnp.concatenate([-sine, sine], axis=1)

    project = pl.pallas_call(
        project_body,
        out_shape=(
            jax.ShapeDtypeStruct((rows + rows // 2, LANES), BF16),
            jax.ShapeDtypeStruct((2 * rows + rows // 2, LANES), BF16),
        ),
        scratch_shapes=[
            pltpu.VMEM((rows, q_latent.shape[1]), BF16),
            pltpu.VMEM((rows, kv_latent.shape[1]), BF16),
            pltpu.VMEM((rows, ROPE_DIM), F32),
        ],
        compiler_params=params(),
        name="project",
    )
    q_own, kv_own = project(
        latent, turn, w_query.T, w_key, w_value, query_gain[None], key_gain[None], cosine, sine
    )

    kv_all = [kv_own] + [move(kv_own, d, 0) for d in (1, 3, 2)]
    q_all = [q_own] + [move(q_own, 0, d) for d in (1, 3, 2)]
    partial = pl.pallas_call(
        attend_body,
        out_shape=[jax.ShapeDtypeStruct((rows + 16, LANES), BF16)] * SIDE,
        scratch_shapes=[pltpu.VMEM((SIDE * rows, 2 * LANES), BF16)] * 3
        + [pltpu.VMEM((SIDE * rows, 2 * LANES), F32)],
        compiler_params=params(),
        name="attend",
    )(*q_all, *kv_all)
    parts = [partial[0]] + [
        move(p, 0, -d) for p, d in zip(partial[1:], (1, 3, 2))
    ]

    picked = []
    for w in (w_down, w_gate, w_up):
        picked.append(lax.dynamic_index_in_dim(w, 1 - core, 0, False))
    down_twin, *twin = [lax.ppermute(w, "tp", swap) for w in picked]
    mix_twin = lax.ppermute(w_mix, "tp", swap)

    step = chips // 2
    hidden = w_gate.shape[2]
    terms = pl.pallas_call(
        expert_body,
        out_shape=jax.ShapeDtypeStruct((chips, slots, width), BF16),
        grid_spec=pltpu.PrefetchScalarGridSpec(
            num_scalar_prefetch=1,
            grid=(chips // step,),
            in_specs=[
                pl.BlockSpec((step, slots, width), lambda j, c: (j, 0, 0)),
                pl.BlockSpec((1, width, hidden), lambda j, c: (c[0], 0, 0)),
                pl.BlockSpec((1, width, hidden), lambda j, c: (c[0], 0, 0)),
                pl.BlockSpec((1, hidden, width), lambda j, c: (c[0], 0, 0)),
                pl.BlockSpec((width, hidden), lambda j, c: (0, 0)),
                pl.BlockSpec((width, hidden), lambda j, c: (0, 0)),
                pl.BlockSpec((hidden, width), lambda j, c: (0, 0)),
            ],
            out_specs=pl.BlockSpec((step, slots, width), lambda j, c: (j, 0, 0)),
        ),
        compiler_params=params(),
        name="experts",
    )(core.reshape(1), everyone, w_gate, w_up, w_down, *twin, down_twin)

    own_head, twin_head = pl.pallas_call(
        join_body,
        out_shape=[jax.ShapeDtypeStruct((half, VALUE_DIM), BF16)] * 2,
        in_specs=[pl.BlockSpec(memory_space=pltpu.SMEM)]
        + [pl.BlockSpec(memory_space=pltpu.VMEM)] * SIDE,
        scratch_shapes=[pltpu.VMEM((rows, VALUE_DIM), BF16)],
        compiler_params=params(),
        name="join",
    )(core.reshape(1), *parts)
    twin_head = lax.ppermute(twin_head, "tp", swap)
    mixed = pl.pallas_call(
        mix_body,
        out_shape=jax.ShapeDtypeStruct((half, width), BF16),
        grid=(2,),
        in_specs=[pl.BlockSpec((half // 2, VALUE_DIM), lambda i: (i, 0))] * 2
        + [pl.BlockSpec((VALUE_DIM, width), lambda i: (0, 0))] * 2,
        out_specs=pl.BlockSpec((half // 2, width), lambda i: (i, 0)),
        compiler_params=params(),
        name="mix",
    )(own_head, twin_head, w_mix, mix_twin)

    def summed(x):
        return lax.psum_scatter(
            x, "tp", scatter_dimension=0, tiled=True, axis_index_groups=same_core
        )

    done = summed(terms.reshape(chips * slots, width))
    mix_out = summed(mixed)
    returned = lax.all_to_all(
        done.reshape(EXPERTS, CAP, width), ("ep", "tp"), 0, 0, axis_index_groups=plane
    )
    expert_out = pl.pallas_call(
        collect_body,
        out_shape=jax.ShapeDtypeStruct((own, width), BF16),
        compiler_params=params(),
        name="collect",
    )(returned, id_rows, route_weights.T)
    return (mix_out, expert_out)


def solution(mesh):
    in_specs = (
        P(("ep", "tp"), None),
        P(("ep", "tp"), None),
        P(("ep", "tp"), None),
        P(),
        P(),
        P(None, "tp"),
        P(None, "tp"),
        P(None, "tp"),
        P(),
        P(),
        P("tp", None),
        P(("ep", "tp"), None),
        P(),
        P(("ep", "tp"), None),
        P(("ep", "tp"), None),
        P("ep", None, "tp"),
        P("ep", None, "tp"),
        P("ep", "tp", None),
    )
    out_specs = (P(("ep", "tp"), None), P(("ep", "tp"), None))

    return jax.shard_map(
        on_device, mesh=mesh, in_specs=in_specs, out_specs=out_specs, check_vma=False
    )
```

```python
import jax
import jax.numpy as jnp
from jax import lax
from jax.experimental import pallas as pl
from jax.experimental.pallas import tpu as pltpu
from jax.sharding import PartitionSpec as P


NOPE_DIM = 128
ROPE_DIM = 64
VALUE_DIM = 128
HEAD_DIM = NOPE_DIM + ROPE_DIM
EXPERTS = 32
TOP_K = 2
CAP = 4
SIDE = 4
EPSILON = 1e-06
THETA = 10000.0
LANES = 128
LOG2E = 1.4426950408889634


BF16 = jnp.bfloat16
F32 = jnp.float32


def params(mib=56):
    return pltpu.CompilerParams(vmem_limit_bytes=mib * 1024 * 1024)


def rms(values, gains):
    return values * lax.rsqrt(jnp.mean(values * values, axis=-1, keepdims=True) + EPSILON) * gains


def latent_body(q_ref, kv_ref, rope_ref, qg_ref, kvg_ref, out_ref):
    rows = q_ref.shape[0]
    q = rms(q_ref[...].astype(F32), qg_ref[...][None, :]).astype(BF16)
    kv = rms(kv_ref[...].astype(F32), kvg_ref[...]).astype(BF16)
    rope = rope_ref[...].astype(F32)
    parts = [p[:, j : j + LANES] for p in (q, kv) for j in range(0, p.shape[1], LANES)]
    packed = jnp.concatenate([rope[: rows // 2, :], rope[rows // 2 :, :]], axis=1)
    for peer in range(out_ref.shape[0]):
        for n, part in enumerate(parts):
            out_ref[peer, n * rows : (n + 1) * rows, :] = part
        out_ref[peer, len(parts) * rows :, :] = packed.astype(BF16)


def square(row):
    return jnp.broadcast_to(row, (row.shape[1], row.shape[1]))


def slots_of(rows, as_rows):
    count = rows.shape[1]
    line = lax.broadcasted_iota(jnp.int32, (count, count), 0)
    lane = lax.broadcasted_iota(jnp.int32, (count, count), 1)
    ids = [square(rows[k : k + 1, :].astype(F32)) for k in range(TOP_K)]
    outs = []
    for k in range(TOP_K):
        if as_rows:
            same = sum(jnp.where((p.T == ids[k]) & (line < lane), 1.0, 0.0) for p in ids)
            picked = ids[k][:1, :] * CAP + jnp.sum(same, axis=0, keepdims=True)
        else:
            mine = ids[k].T
            same = sum(jnp.where((p == mine) & (lane < line), 1.0, 0.0) for p in ids)
            picked = mine[:, :1] * CAP + jnp.sum(same, axis=1, keepdims=True)
        outs.append(picked.astype(jnp.int32))
    return outs


def dispatch_body(tok_ref, gain_ref, rows_ref, out_ref):
    normed = rms(tok_ref[...].astype(F32), gain_ref[...]).astype(BF16)
    first, second = slots_of(rows_ref[...], True)
    experts, cap, width = out_ref.shape
    shape = (experts * cap, normed.shape[0])
    slot = lax.broadcasted_iota(jnp.int32, shape, 0)
    hot = jnp.where((slot == first) | (slot == second), 1.0, 0.0).astype(BF16)
    picked = jnp.dot(hot, normed, preferred_element_type=F32)
    out_ref[...] = picked.reshape(experts, cap, width).astype(BF16)


def collect_body(back_ref, rows_ref, weight_ref, out_ref):
    first, second = slots_of(rows_ref[...], False)
    count = out_ref.shape[0]
    slots = back_ref.shape[0] * back_ref.shape[1]
    slot = lax.broadcasted_iota(jnp.int32, (count, slots), 1)
    weights = [square(weight_ref[k : k + 1, :]).T[:, :1] for k in range(TOP_K)]
    mixed = jnp.where(slot == first, weights[0], 0.0) + jnp.where(slot == second, weights[1], 0.0)
    high = mixed.astype(BF16)
    rest = mixed - high.astype(F32)
    low = rest.astype(BF16)
    last = (rest - low.astype(F32)).astype(BF16)
    back = back_ref[...].astype(F32).reshape(slots, back_ref.shape[2]).astype(BF16)
    total = jnp.dot(high, back, preferred_element_type=F32)
    total += jnp.dot(low, back, preferred_element_type=F32)
    total += jnp.dot(last, back, preferred_element_type=F32)
    out_ref[...] = total.astype(BF16)


def turned(values, cosine, sine):
    half = values.shape[-1] // 2
    swapped = jnp.concatenate([values[:, half:], values[:, :half]], axis=1)
    return values * cosine + swapped * sine


def project_body(
    mine_ref, other_ref, wq_ref, wk_ref, wv_ref, qg_ref, kg_ref, cos_ref, sin_ref,
    q_ref, kv_ref, lat_q, lat_kv,
):
    groups, height, _ = mine_ref.shape
    q_parts = lat_q.shape[1] // LANES
    kv_parts = lat_kv.shape[1] // LANES
    own = 2 * height // (2 * (q_parts + kv_parts) + 1)
    half = groups * own
    ropes = []
    for n, src in enumerate((mine_ref, other_ref)):
        for j in range(q_parts + kv_parts):
            piece = src[:, j * own : (j + 1) * own, :].reshape(half, LANES)
            dst, col = (lat_q, j) if j < q_parts else (lat_kv, j - q_parts)
            dst[n * half : (n + 1) * half, col * LANES : (col + 1) * LANES] = piece
        packed = src[:, (q_parts + kv_parts) * own :, :].astype(F32)
        pair = [packed[:, :, :ROPE_DIM], packed[:, :, ROPE_DIM:]]
        ropes.append(jnp.concatenate(pair, axis=1).reshape(half, ROPE_DIM))
    rope = jnp.concatenate(ropes, axis=0)
    cosine, sine = cos_ref[...], sin_ref[...]
    queries = lax.dot_general(
        lat_q[...], wq_ref[...], (((1,), (1,)), ((), ())), preferred_element_type=F32
    )
    scale = HEAD_DIM**-0.5 * LOG2E
    queries = rms(queries, qg_ref[...] * scale)
    q_ref[: 2 * half, :] = queries[:, :NOPE_DIM].astype(BF16)
    q_rope = turned(queries[:, NOPE_DIM:], cosine, sine).astype(BF16)
    q_ref[2 * half :, :] = jnp.concatenate([q_rope[:half], q_rope[half:]], axis=1)
    latent = lat_kv[...]
    keys = jnp.dot(latent, wk_ref[...], preferred_element_type=F32)
    square = jnp.sum(keys * keys, axis=-1, keepdims=True) + jnp.sum(
        rope * rope, axis=-1, keepdims=True
    )
    factor = lax.rsqrt(square / HEAD_DIM + EPSILON)
    gains = kg_ref[...]
    kv_ref[: 2 * half, :] = (keys * factor * gains[:, :NOPE_DIM]).astype(BF16)
    kv_ref[2 * half : 4 * half, :] = jnp.dot(
        latent, wv_ref[...], preferred_element_type=F32
    ).astype(BF16)
    k_rope = turned(rope * factor * gains[:, NOPE_DIM:], cosine, sine).astype(BF16)
    kv_ref[4 * half :, :] = jnp.concatenate([k_rope[:half], k_rope[half:]], axis=1)


def attend_body(*refs):
    q_refs, kv_refs, out_refs = refs[:SIDE], refs[SIDE : 2 * SIDE], refs[2 * SIDE : 3 * SIDE]
    qs, ks, vs, acc_ref = refs[3 * SIDE :]
    rows = qs.shape[0] // SIDE
    half = rows // 2
    zero = jnp.zeros((half, ROPE_DIM), BF16)
    ones = jnp.ones((rows, LANES), BF16)
    for b in range(SIDE):
        at = b * rows
        for src, dst, off in ((q_refs[b], qs, rows), (kv_refs[b], ks, 2 * rows)):
            dst[at : at + rows, :NOPE_DIM] = src[:rows, :]
            packed = src[off : off + half, :]
            dst[at : at + half, NOPE_DIM:] = jnp.concatenate([packed[:, :ROPE_DIM], zero], axis=1)
            dst[at + half : at + rows, NOPE_DIM:] = jnp.concatenate(
                [packed[:, ROPE_DIM:], zero], axis=1
            )
        vs[at : at + rows, :VALUE_DIM] = kv_refs[b][rows : 2 * rows, :]
        vs[at : at + rows, VALUE_DIM:] = ones

    def block(i, carry):
        here = pl.ds(pl.multiple_of(i * rows, rows), rows)
        q = qs[here, :]
        acc = None
        for b in range(SIDE):
            there = slice(b * rows, (b + 1) * rows)
            scores = lax.dot_general(
                q, ks[there, :], (((1,), (1,)), ((), ())), preferred_element_type=F32
            )
            probs = jnp.exp2(scores).astype(BF16)
            term = jnp.dot(probs, vs[there, :], preferred_element_type=F32)
            acc = term if acc is None else acc + term
        acc_ref[here, :] = acc
        return carry

    lax.fori_loop(0, SIDE, block, 0)
    for b in range(SIDE):
        at = b * rows
        out_refs[b][:rows, :] = acc_ref[at : at + rows, :VALUE_DIM].astype(BF16)
        for j in range(rows // LANES):
            total = acc_ref[at + j * LANES : at + (j + 1) * LANES, VALUE_DIM:].T[0:1, :]
            high = total.astype(BF16)
            low = (total - high.astype(F32)).astype(BF16)
            out_refs[b][rows + j : rows + j + 1, :] = high
            out_refs[b][rows + 8 + j : rows + 8 + j + 1, :] = low


def join_body(*refs):
    parts, outs = refs[:SIDE], refs[SIDE:]
    half = outs[0].shape[0]
    rows = 2 * half
    total = sum(
        p[rows : rows + 8, :].astype(F32) + p[rows + 8 : rows + 16, :].astype(F32) for p in parts
    )
    inverse = 1.0 / total
    for j in range(rows // LANES):
        there = slice(j * LANES, (j + 1) * LANES)
        scale = jnp.broadcast_to(inverse[j : j + 1, :], (LANES, LANES)).T
        head = sum(p[there, :].astype(F32) for p in parts)
        at = j * LANES % half
        outs[j * LANES // half][at : at + LANES, :] = (head * scale).astype(BF16)


def mix_body(own_ref, twin_ref, w_own_ref, w_twin_ref, out_ref):
    term = jnp.dot(own_ref[...], w_own_ref[...], preferred_element_type=F32)
    term += jnp.dot(twin_ref[...], w_twin_ref[...], preferred_element_type=F32)
    out_ref[...] = term.astype(BF16)


def expert_body(core_ref, x_ref, *refs):
    sources, out_ref, held, sems = refs[:6], refs[6], refs[7:13], refs[13]
    groups, rows, width = x_ref.shape
    first = pl.program_id(0) == 0
    views = [r.at[core_ref[0]] for r in sources[:3]] + list(sources[3:])
    copies = [
        pltpu.make_async_copy(view, dst, sems.at[n]) for n, (view, dst) in enumerate(zip(views, held))
    ]

    @pl.when(first)
    def _():
        for copy in copies:
            copy.start()

    def weights(n):
        @pl.when(first)
        def _():
            copies[n].wait()

        return held[n][...]

    x = x_ref[...].reshape(groups * rows, width)
    out = None
    for n in (0, 3):
        gate = jnp.dot(x, weights(n), preferred_element_type=F32)
        up = jnp.dot(x, weights(n + 1), preferred_element_type=F32)
        hidden = (gate / (1.0 + jnp.exp(-gate)) * up).astype(BF16)
        term = jnp.dot(hidden, weights(n + 2), preferred_element_type=F32)
        out = term if out is None else out + term
    out_ref[...] = out.astype(BF16).reshape(groups, rows, width)


def shift(keys, queries, tp_count):
    pairs = []
    for e in range(SIDE * SIDE):
        for t in range(tp_count):
            step_x, step_y = (keys, queries) if t % 2 == 0 else (queries, keys)
            there = (e // SIDE + step_y) % SIDE * SIDE + (e % SIDE + step_x) % SIDE
            pairs.append((e * tp_count + t, there * tp_count + t))
    return pairs


def on_device(
    q_latent,
    kv_latent,
    rope_key,
    q_latent_gain,
    kv_latent_gain,
    w_query,
    w_key,
    w_value,
    query_gain,
    key_gain,
    w_mix,
    tokens_b,
    norm_gain,
    expert_ids,
    route_weights,
    w_gate,
    w_up,
    w_down,
):
    tp_count = lax.axis_size("tp")
    ep_count = lax.axis_size("ep")
    chips = tp_count // 2
    own = q_latent.shape[0]
    rows = own * tp_count
    half = rows // 2
    width = tokens_b.shape[1]
    slots = EXPERTS * CAP
    tp_at = lax.axis_index("tp")
    core = tp_at % 2
    same_core = [[z * 2 + c for z in range(chips)] for c in range(2)]
    plane = [
        [e * tp_count + z * 2 + c for e in range(ep_count) for c in range(2)] for z in range(chips)
    ]
    swap = [(i, i ^ 1) for i in range(tp_count)]

    def move(x, keys, queries):
        return lax.ppermute(x, ("ep", "tp"), shift(keys, queries, tp_count))


    height = own * ((q_latent.shape[1] + kv_latent.shape[1]) // LANES) + own // 2
    latents = pl.pallas_call(
        latent_body,
        out_shape=jax.ShapeDtypeStruct((chips, height, LANES), BF16),
        compiler_params=params(),
        name="latents",
    )
    latent = latents(q_latent, kv_latent, rope_key, q_latent_gain, kv_latent_gain[None])

    id_rows = expert_ids.T
    dispatch = pl.pallas_call(
        dispatch_body,
        out_shape=jax.ShapeDtypeStruct((EXPERTS, CAP, width), BF16),
        compiler_params=params(),
        name="dispatch",
    )
    outgoing = dispatch(tokens_b, norm_gain[None], id_rows)

    arrived = lax.all_to_all(
        outgoing, ("ep", "tp"), 0, 0, axis_index_groups=plane
    )
    everyone = lax.all_gather(
        arrived.reshape(slots, width), "tp", axis=0, axis_index_groups=same_core
    )

    mine = lax.all_to_all(latent, "tp", 0, 0, axis_index_groups=same_core)
    other = lax.ppermute(mine, "tp", swap)

    block = jnp.arange(rows, dtype=jnp.int32) // own
    side = jnp.where(block < chips, core, 1 - core)
    positions = (
        lax.axis_index("ep") * rows
        + ((block % chips) * 2 + side) * own
        + jnp.arange(rows, dtype=jnp.int32) % own
    )
    inverse = THETA ** (-jnp.arange(0, ROPE_DIM, 2, dtype=F32) / ROPE_DIM)
    angles = positions.astype(F32)[:, None] * inverse[None, :]
    cosine, sine = jnp.cos(angles), jnp.sin(angles)
    cosine = jnp.concatenate([cosine, cosine], axis=1)
    sine = jnp.concatenate([-sine, sine], axis=1)

    project = pl.pallas_call(
        project_body,
        out_shape=(
            jax.ShapeDtypeStruct((rows + rows // 2, LANES), BF16),
            jax.ShapeDtypeStruct((2 * rows + rows // 2, LANES), BF16),
        ),
        scratch_shapes=[
            pltpu.VMEM((rows, q_latent.shape[1]), BF16),
            pltpu.VMEM((rows, kv_latent.shape[1]), BF16),
        ],
        compiler_params=params(),
        name="project",
    )
    q_own, kv_own = project(
        mine, other, w_query.T, w_key, w_value, query_gain[None], key_gain[None], cosine, sine
    )

    kv_all = [kv_own] + [move(kv_own, d, 0) for d in (1, 3, 2)]
    q_all = [q_own] + [move(q_own, 0, d) for d in (1, 3, 2)]
    partial = pl.pallas_call(
        attend_body,
        out_shape=[jax.ShapeDtypeStruct((rows + 16, LANES), BF16)] * SIDE,
        scratch_shapes=[pltpu.VMEM((SIDE * rows, 2 * LANES), BF16)] * 3
        + [pltpu.VMEM((SIDE * rows, 2 * LANES), F32)],
        compiler_params=params(),
        name="attend",
    )(*q_all, *kv_all)
    parts = [partial[0]] + [
        move(p, 0, -d) for p, d in zip(partial[1:], (1, 3, 2))
    ]

    picked = []
    for w in (w_down, w_gate, w_up):
        picked.append(lax.dynamic_index_in_dim(w, 1 - core, 0, False))
    down_twin, *twin = [lax.ppermute(w, "tp", swap) for w in picked]
    mix_twin = lax.ppermute(w_mix, "tp", swap)

    step = chips // 2
    hidden = w_gate.shape[2]
    terms = pl.pallas_call(
        expert_body,
        out_shape=jax.ShapeDtypeStruct((chips, slots, width), BF16),
        grid_spec=pltpu.PrefetchScalarGridSpec(
            num_scalar_prefetch=1,
            grid=(chips // step,),
            in_specs=[
                pl.BlockSpec((step, slots, width), lambda j, c: (j, 0, 0)),
            ]
            + [pl.BlockSpec(memory_space=pl.ANY)] * 6,
            scratch_shapes=[
                pltpu.VMEM(shape, BF16)
                for shape in ((width, hidden), (width, hidden), (hidden, width)) * 2
            ]
            + [pltpu.SemaphoreType.DMA((6,))],
            out_specs=pl.BlockSpec((step, slots, width), lambda j, c: (j, 0, 0)),
        ),
        compiler_params=params(),
        name="experts",
    )(core.reshape(1), everyone, w_gate, w_up, w_down, *twin, down_twin)

    own_head, twin_head = pl.pallas_call(
        join_body,
        out_shape=[jax.ShapeDtypeStruct((half, VALUE_DIM), BF16)] * 2,
        compiler_params=params(),
        name="join",
    )(*parts)
    twin_head = lax.ppermute(twin_head, "tp", swap)
    mixed = pl.pallas_call(
        mix_body,
        out_shape=jax.ShapeDtypeStruct((half, width), BF16),
        grid=(2,),
        in_specs=[pl.BlockSpec((half // 2, VALUE_DIM), lambda i: (i, 0))] * 2
        + [pl.BlockSpec((VALUE_DIM, width), lambda i: (0, 0))] * 2,
        out_specs=pl.BlockSpec((half // 2, width), lambda i: (i, 0)),
        compiler_params=params(),
        name="mix",
    )(own_head, twin_head, w_mix, mix_twin)

    def summed(x):
        return lax.psum_scatter(
            x, "tp", scatter_dimension=0, tiled=True, axis_index_groups=same_core
        )

    done = summed(terms.reshape(chips * slots, width))
    mix_out = summed(mixed)
    returned = lax.all_to_all(
        done.reshape(EXPERTS, CAP, width), ("ep", "tp"), 0, 0, axis_index_groups=plane
    )
    expert_out = pl.pallas_call(
        collect_body,
        out_shape=jax.ShapeDtypeStruct((own, width), BF16),
        compiler_params=params(),
        name="collect",
    )(returned, id_rows, route_weights.T)
    return (mix_out, expert_out)


def solution(mesh):
    in_specs = (
        P(("ep", "tp"), None),
        P(("ep", "tp"), None),
        P(("ep", "tp"), None),
        P(),
        P(),
        P(None, "tp"),
        P(None, "tp"),
        P(None, "tp"),
        P(),
        P(),
        P("tp", None),
        P(("ep", "tp"), None),
        P(),
        P(("ep", "tp"), None),
        P(("ep", "tp"), None),
        P("ep", None, "tp"),
        P("ep", None, "tp"),
        P("ep", "tp", None),
    )
    out_specs = (P(("ep", "tp"), None), P(("ep", "tp"), None))

    return jax.shard_map(
        on_device, mesh=mesh, in_specs=in_specs, out_specs=out_specs, check_vma=False
    )
```
